32 devices in a mesh: ep: 4 (over y, x), tp: 8 (over z, core).
Axes of the slice: x: 2, y: 2, z: 4, core: 2. Of those that a mesh axis runs over, the one named last changes fastest.
Arguments:
- mixer_input_channels: bfloat16 [8192, 2048], P('ep', 'tp'), may hold values from -6 to 6
- output_gate_logits: bfloat16 [8192, 2048], P('ep', 'tp'), may hold values from -6 to 6
- head_group_input_map: bfloat16 [8192, 256], P('ep'), may hold values from -6 to 6
- head_group_output_map: bfloat16 [8192, 256], P('ep'), may hold values from -6 to 6
- input_channel_taps: bfloat16 [4, 2048], P(None, 'tp'), may hold values from -3 to 3
- input_map_taps: bfloat16 [4, 256], replicated, may hold values from -3 to 3
- output_map_taps: bfloat16 [4, 256], replicated, may hold values from -3 to 3
- step_logits: float32 [32, 8192], P('tp', 'ep'), may hold values from -5 to 5
- head_log_rate: float32 [32], P('tp'), may hold values from -20 to -2
- extra_log_decay: float32 [32, 8192], P('tp', 'ep'), may hold values from -1 to 0
- head_direct_scale: float32 [32], P('tp'), may hold values from 1 to 6
- gated_norm_scale: bfloat16 [2048], P('tp'), may hold values from 0.099609375 to 1.8984375
- mixer_output_weight: bfloat16 [2048, 2048], P('tp'), may hold values from -0.125 to 0.125
- second_batch_tokens: bfloat16 [1024, 2048], P('ep'), may hold values from -6 to 6
- pre_expert_norm_scale: bfloat16 [2048], replicated, may hold values from 0.099609375 to 1.8984375
- group_router_columns: bfloat16 [2048, 1], replicated
- expert_router_columns: bfloat16 [2048, 4], replicated
- routes: int32 [1024, 2], P('ep'), may hold values from 0 to 3, all different within a row; in each aligned block of 256 rows (0 to 255, 256 to 511, ...) at most 256 rows name the same one
- expert_gate_weight: bfloat16 [4, 2048, 4096], P('ep', None, 'tp'), may hold values from -0.125 to 0.125
- expert_up_weight: bfloat16 [4, 2048, 4096], P('ep', None, 'tp'), may hold values from -0.125 to 0.125
- expert_down_weight: bfloat16 [4, 4096, 2048], P('ep', 'tp'), may hold values from -0.125 to 0.125
Outputs:
- mixer_out: bfloat16 [8192, 2048], P(('ep', 'tp'))
- experts_out: bfloat16 [1024, 2048], P('ep', 'tp')
The draws below stay inside these ranges and needn't reach their ends.
Inputs may be any that keep to these rules, and one draw needn't show every extreme that they name: `routes`: in each aligned block of 256 rows no expert is named more than 256 times, some expert exactly 256 times in some block; a row's two experts differ.
All inputs are finite; a program needn't handle non-finite values.
Results may differ from the reference program's by a relative error of at most 0.019.
Values may be sent and summed in bfloat16 or wider, within the bound.
A program may use at most 128 MiB of HBM per device.

```python
import math
import jax
import jax.numpy as jnp
import numpy as np
from jax import lax

D = 2048
HEADS = 32
HEAD_DIM = 64
STATE = 64
GROUPS = 4
CONV = 4
BLOCK = 128
FF = 4096
TOK_SHARD = 2048
TOKB = 256
INNER = 2048
SEQ = 8192
TOKENS = 1024
EXPERTS = 4
EXPERT_GROUPS = 1
CAP = 256
FF_SHARD = 512
N_EP = 4
N_TP = 8


def draw_step_logits(key, part):
    first, second = jax.random.split(jax.random.fold_in(key, 11))
    span = max(TOK_SHARD // 2, 1)
    offset = jax.random.uniform(second, (HEADS, SEQ // span), jnp.float32, -1.5, 1.5)
    offset = jnp.repeat(offset, span, axis=1)
    noise = jnp.clip(jax.random.normal(first, (HEADS, SEQ), jnp.float32), -3.0, 3.0)
    return (noise + offset).astype(jnp.float32)


def draw_head_log_rate(key, part):
    first, second, third = jax.random.split(jax.random.fold_in(key, 12), 3)
    share = 0.5
    quick = jax.random.uniform(first, (HEADS,), jnp.float32) < share
    quick_rate = jax.random.uniform(second, (HEADS,), jnp.float32, math.log(0.02), math.log(0.1))
    slow_rate = jax.random.uniform(third, (HEADS,), jnp.float32, math.log(0.3), math.log(2.3)) - math.log(SEQ)
    return jnp.where(quick, quick_rate, slow_rate).astype(jnp.float32)


def draw_extra_log_decay(key, part):
    first, second = jax.random.split(jax.random.fold_in(key, 13))
    struck = jax.random.uniform(first, (HEADS, SEQ), jnp.float32) < 6.0 / SEQ
    depth = jax.random.uniform(second, (HEADS, SEQ), jnp.float32, math.log(0.5), math.log(0.8))
    return jnp.where(struck, depth, 0.0).astype(jnp.float32)


def router_columns(key, columns):
    first = jax.random.fold_in(key, 0)
    base = jax.random.normal(first, (D, columns), jnp.float32) / math.sqrt(D)
    return base.astype(jnp.bfloat16)


def draw_group_router_columns(key, part):
    return router_columns(jax.random.fold_in(key, 14), EXPERT_GROUPS)


def draw_expert_router_columns(key, part):
    return router_columns(jax.random.fold_in(key, 15), EXPERTS)


def spiked(result, stream_key, source, target, shards_of, factor):
    owner, partner = [(jnp.arange(result.shape[position]) // (result.shape[position] // shards_of)).reshape([-1 if axis == position else 1 for axis in range(result.ndim)]) for position in (source, target)]
    chosen = jax.random.permutation(stream_key, shards_of)[partner]
    strong = (owner == chosen) | (owner == (partner + shards_of // 2) % shards_of)
    return jnp.where(strong, factor * result, result)


def block_levels(stream_key, extent, cuts, low, high):
    def one(axis_at, blocks):
        draws = jax.random.uniform(jax.random.fold_in(jax.random.fold_in(stream_key, 6), axis_at), (blocks,), jnp.float32, low / len(cuts), high / len(cuts))
        return jnp.repeat(jnp.exp(draws), extent[axis_at] // blocks).reshape((-1,) + (1,) * (len(extent) - axis_at - 1))

    gain = one(*cuts[0])
    for cut in cuts[1:]:
        gain = gain * one(*cut)
    return gain


def deal_out(stream_key, own, number, rows, amount, top, bound, skew):
    order = jax.random.permutation(stream_key, amount)
    packed, common = load_shares(amount, rows * top, bound, skew, True), load_shares(amount, rows * top, bound, skew, False)
    places = jnp.arange(amount)

    def named(sizes, turn):
        used = int((sizes > 0).sum())
        fixed = max(1, used // 4)
        moved = fixed + (places - fixed + turn * (used - fixed)) % max(1, amount - fixed)
        return jnp.zeros((amount,), jnp.int32).at[order[jnp.where(places < fixed, places, moved)]].set(jnp.asarray(sizes, jnp.int32))

    sizes = jnp.where(number % 4 == 0, named(packed, number // 4), named(common, number - number // 4 - 1))
    mixed = jax.random.permutation(jax.random.fold_in(own, 3), amount)
    donor, taker = mixed[0:amount // 2 * 2:2], mixed[1:amount // 2 * 2:2]
    margin = jnp.minimum(sizes[donor] - 1, bound - sizes[taker]) // 2
    margin = jnp.where((donor == order[0]) | (taker == order[0]) | (sizes[taker] == 0), 0, jnp.maximum(margin, 0))
    moved = jax.random.randint(jax.random.fold_in(own, 4), (amount // 2,), 0, 1 << 20) % (margin + 1)
    sizes = sizes.at[donor].add(-moved).at[taker].add(moved)
    members = jnp.searchsorted(jnp.cumsum(sizes), jnp.arange(rows * top), side="right").astype(jnp.int32)
    grid = members.reshape(top, rows).T
    grid = grid[jax.random.permutation(jax.random.fold_in(own, 1), rows)]
    turn = jax.random.randint(jax.random.fold_in(own, 2), (rows, 1), 0, top)
    return jnp.take_along_axis(grid, (jnp.arange(top)[None, :] + turn) % top, axis=1)


def load_shares(number_of, total, limit, skew, full):
    loads = [(1 << 20) // math.isqrt(rank ** skew) + 1 for rank in range(1, number_of + 1)]
    largest = limit if full else min(limit, max(-(-total // number_of), total * loads[0] // sum(loads)))
    least = 1 if total - largest >= number_of - 1 else 0
    given, spare = [largest] + [least] * (number_of - 1), total - largest - least * (number_of - 1)
    while spare > 0:
        free = [i for i in range(1, number_of) if given[i] < largest] or [i for i in range(1, number_of) if given[i] < limit]
        whole, left = sum([loads[i] for i in free]), spare
        for i in free:
            more = min(limit - given[i], max(1, left * loads[i] // whole), spare)
            given[i] = given[i] + more
            spare = spare - more
    return np.array(given)


def bell_draw(key, shape, spread, most, cuts=(), kind=jnp.bfloat16):
    entries = jax.random.normal(key, shape, jnp.float32) * spread
    if len(cuts) > 0:
        entries = block_levels(key, shape, cuts, -0.22, 0.18) * entries
    return jnp.clip(entries, min=-most, max=most).astype(kind)


def noise_with(key, extent, deviation, reach, shards, heavy, kind=jnp.bfloat16):
    result = deviation * jax.random.normal(key, extent, jnp.float32)
    if shards:
        result = result * block_levels(key, extent, shards, -0.22, 0.18)
    return jnp.clip(spiked(result, jax.random.fold_in(key, 3), *heavy), -reach, reach).astype(kind)


def setup_inputs(seed: int = 0) -> dict:
    splits = jax.random.split(jax.random.key(seed), 22)
    mixer_input_channels = bell_draw(splits[0], (SEQ, INNER), 1.0, 6.0, ((0, 4), (1, 8)))
    output_gate_logits = bell_draw(splits[1], (SEQ, INNER), 1.0, 6.0, ((0, 4), (1, 8)))
    head_group_input_map = bell_draw(splits[2], (SEQ, GROUPS * STATE), 1.0, 6.0, ((0, 4),))
    head_group_output_map = bell_draw(splits[3], (SEQ, GROUPS * STATE), 1.0, 6.0, ((0, 4),))
    input_channel_taps = bell_draw(splits[4], (CONV, INNER), CONV ** -0.5, 3.0, ((1, 8),))
    input_map_taps = bell_draw(splits[5], (CONV, GROUPS * STATE), CONV ** -0.5, 3.0)
    output_map_taps = bell_draw(splits[6], (CONV, GROUPS * STATE), CONV ** -0.5, 3.0)
    step_logits = draw_step_logits(jax.random.fold_in(splits[21], 71), 0)
    head_log_rate = draw_head_log_rate(jax.random.fold_in(splits[21], 71), 0)
    extra_log_decay = draw_extra_log_decay(jax.random.fold_in(splits[21], 71), 0)
    head_direct_scale = jnp.clip(1.0 + 5.0 * jax.random.uniform(splits[10], (HEADS,), jnp.float32) ** block_levels(splits[10], (HEADS,), ((0, 8),), -0.2, 0.2), 1.0, 6.0)
    gated_norm_scale = jnp.clip(1.0 + 0.18 * jax.random.normal(splits[11], (INNER,), jnp.float32), 0.099609375, 1.8984375).astype(jnp.bfloat16)
    mixer_output_weight = bell_draw(splits[12], (INNER, D), INNER ** -0.5, 0.125, ((0, 8),))
    second_batch_tokens = bell_draw(splits[13], (TOKENS, D), 1.0, 6.0, ((0, 4),))
    pre_expert_norm_scale = jnp.clip(1.0 + 0.18 * jax.random.normal(splits[14], (D,), jnp.float32), 0.099609375, 1.8984375).astype(jnp.bfloat16)
    group_router_columns = draw_group_router_columns(jax.random.fold_in(splits[21], 71), 0)
    expert_router_columns = draw_expert_router_columns(jax.random.fold_in(splits[21], 71), 0)
    routes_keys = jax.random.split(jax.random.fold_in(splits[17], 1), TOKENS // TOKB)
    routes_turns = jax.random.permutation(jax.random.fold_in(splits[17], 3), TOKENS // TOKB)
    routes = jax.vmap(lambda own, number: deal_out(jax.random.fold_in(splits[17], 2), own, number, TOKB, EXPERTS, 2, CAP, 2))(routes_keys, routes_turns).reshape((TOKENS, 2))
    expert_gate_weight = bell_draw(splits[18], (EXPERTS, D, FF), D ** -0.5, 0.125, ((0, 4), (2, 8)))
    expert_up_weight = bell_draw(splits[19], (EXPERTS, D, FF), D ** -0.5, 0.125, ((0, 4), (2, 8)))
    expert_down_weight = noise_with(splits[20], (EXPERTS, FF, D), FF ** -0.5, 0.125, ((0, 4), (1, 8)), (1, 2, 8, 2.0))
    return {"mixer_input_channels": mixer_input_channels, "output_gate_logits": output_gate_logits, "head_group_input_map": head_group_input_map, "head_group_output_map": head_group_output_map, "input_channel_taps": input_channel_taps, "input_map_taps": input_map_taps, "output_map_taps": output_map_taps, "step_logits": step_logits, "head_log_rate": head_log_rate, "extra_log_decay": extra_log_decay, "head_direct_scale": head_direct_scale, "gated_norm_scale": gated_norm_scale, "mixer_output_weight": mixer_output_weight, "second_batch_tokens": second_batch_tokens, "pre_expert_norm_scale": pre_expert_norm_scale, "group_router_columns": group_router_columns, "expert_router_columns": expert_router_columns, "routes": routes, "expert_gate_weight": expert_gate_weight, "expert_up_weight": expert_up_weight, "expert_down_weight": expert_down_weight}


eps = 1e-06
exact_prec = lax.Precision.HIGHEST

def causal_conv(joined, taps):
    width = taps.shape[0]
    length = joined.shape[0]
    padded = jnp.pad(joined.astype(jnp.float32), ((width - 1, 0), (0, 0)))
    total = jnp.zeros((length, joined.shape[1]), jnp.float32)
    for j in range(width):
        total = total + taps[j].astype(jnp.float32) * padded[j:j + length]
    return jax.nn.silu(total).astype(jnp.bfloat16)

def slot_positions(route_rows, n_experts):
    flat = route_rows.reshape(-1)
    onehot = (flat[:, None] == jnp.arange(n_experts, dtype=jnp.int32)[None, :]).astype(jnp.int32)
    return (lax.optimization_barrier(jnp.sum(onehot * jnp.cumsum(onehot, axis=0), axis=1)) - 1).astype(jnp.int32)

def route_weights(group_logits, expert_logits, routes):
    n_groups = group_logits.shape[1]
    n_experts = expert_logits.shape[1]
    per_group = n_experts // n_groups
    group_lp = jax.nn.log_softmax(group_logits, axis=-1)
    inner_lp = jax.nn.log_softmax(expert_logits.reshape(-1, n_groups, per_group), axis=-1).reshape(-1, n_experts)
    total = jnp.repeat(group_lp, per_group, axis=1) + inner_lp
    pick = routes[:, :, None] == jnp.arange(n_experts, dtype=jnp.int32)[None, None, :]
    chosen = lax.optimization_barrier(jnp.sum(jnp.where(pick, total[:, None, :], 0.0), axis=-1))
    return jax.nn.softmax(chosen, axis=-1)

def expert_apply(items):
    rows, gate_w, up_w, down_w = items
    gate = jnp.dot(rows, gate_w, preferred_element_type=jnp.float32)
    upper = jnp.dot(rows, up_w, preferred_element_type=jnp.float32)
    hidden = (jax.nn.silu(gate) * upper).astype(jnp.bfloat16)
    parts = hidden.reshape(rows.shape[0], N_TP, FF_SHARD).astype(jnp.float32)
    down_parts = down_w.reshape(N_TP, FF_SHARD, D).astype(jnp.float32)
    partial_sums = jnp.einsum('rjf,jfd->jrd', parts, down_parts).astype(jnp.bfloat16)
    return lax.optimization_barrier(jnp.sum(partial_sums.astype(jnp.float32), axis=0)).astype(jnp.bfloat16)

def reference(mixer_input_channels, output_gate_logits, head_group_input_map, head_group_output_map, input_channel_taps, input_map_taps, output_map_taps, step_logits, head_log_rate, extra_log_decay, head_direct_scale, gated_norm_scale, mixer_output_weight, second_batch_tokens, pre_expert_norm_scale, group_router_columns, expert_router_columns, routes, expert_gate_weight, expert_up_weight, expert_down_weight):
    joined = jnp.concatenate([mixer_input_channels, head_group_input_map, head_group_output_map], axis=1)
    taps = jnp.concatenate([input_channel_taps, input_map_taps, output_map_taps], axis=1)
    conv = causal_conv(joined, taps)
    xs = conv[:, :INNER]
    bs = conv[:, INNER:INNER + GROUPS * STATE]
    cs = conv[:, INNER + GROUPS * STATE:]
    time_step = jax.nn.softplus(step_logits)
    position_log_decay = extra_log_decay - time_step * jnp.exp(head_log_rate)[:, None]
    per_group = HEADS // GROUPS
    xs_f = xs.astype(jnp.float32).reshape(SEQ, HEADS, HEAD_DIM)
    x_dt = xs_f * jnp.transpose(time_step)[:, :, None]
    bs_h = jnp.repeat(bs.astype(jnp.float32).reshape(SEQ, GROUPS, STATE), per_group, axis=1)
    cs_h = jnp.repeat(cs.astype(jnp.float32).reshape(SEQ, GROUPS, STATE), per_group, axis=1)
    nblk = SEQ // BLOCK
    items = (x_dt.reshape(nblk, BLOCK, HEADS, HEAD_DIM), bs_h.reshape(nblk, BLOCK, HEADS, STATE), cs_h.reshape(nblk, BLOCK, HEADS, STATE), jnp.transpose(position_log_decay).reshape(nblk, BLOCK, HEADS))
    lower = jnp.tril(jnp.ones((BLOCK, BLOCK), bool))[:, :, None]

    def one_block(state, item):
        xb, bb, cb, lb = item
        cum = jnp.cumsum(lb, axis=0)
        diff = cum[:, None, :] - cum[None, :, :]
        weight = jnp.where(lower, jnp.exp(jnp.where(lower, diff, 0.0)), 0.0)
        scores = jnp.einsum('lhn,shn->lsh', cb, bb, precision=exact_prec)
        inner = jnp.einsum('lsh,shp->lhp', scores * weight, xb, precision=exact_prec)
        carried = jnp.einsum('lhn,hpn->lhp', cb, state, precision=exact_prec) * jnp.exp(cum)[:, :, None]
        tail = jnp.exp(cum[-1:] - cum)
        new_state = state * jnp.exp(cum[-1])[:, None, None] + jnp.einsum('shp,shn->hpn', xb * tail[:, :, None], bb, precision=exact_prec)
        return (new_state, inner + carried)
    start = jnp.zeros((HEADS, HEAD_DIM, STATE), jnp.float32)
    _, ssm = lax.scan(one_block, start, items)
    ssm = ssm.reshape(SEQ, HEADS, HEAD_DIM)
    gated = (ssm + head_direct_scale[None, :, None] * xs_f) * jax.nn.silu(output_gate_logits.astype(jnp.float32)).reshape(SEQ, HEADS, HEAD_DIM)
    gated = gated * lax.rsqrt(lax.optimization_barrier(jnp.mean(gated * gated, axis=-1, keepdims=True)) + eps)
    mixed = (gated.reshape(SEQ, INNER) * gated_norm_scale.astype(jnp.float32)).astype(jnp.bfloat16)
    mixer_out = jnp.dot(mixed, mixer_output_weight, preferred_element_type=jnp.float32).astype(jnp.bfloat16)
    tokens_f = second_batch_tokens.astype(jnp.float32)
    normed = (tokens_f * lax.rsqrt(lax.optimization_barrier(jnp.mean(tokens_f * tokens_f, axis=-1, keepdims=True)) + eps) * pre_expert_norm_scale.astype(jnp.float32)).astype(jnp.bfloat16)
    group_logits = jnp.dot(normed, group_router_columns, preferred_element_type=jnp.float32)
    expert_logits = jnp.dot(normed, expert_router_columns, preferred_element_type=jnp.float32)
    weights = route_weights(group_logits, expert_logits, routes)
    block_routes = routes.reshape(N_EP, TOKB, 2)
    positions = jax.vmap(lambda rows: slot_positions(rows, EXPERTS))(block_routes)
    slots = (block_routes.reshape(N_EP, TOKB * 2) * CAP + positions).astype(jnp.int32)
    token_ids = jnp.repeat(jnp.arange(TOKB, dtype=jnp.int32), 2)
    source = jnp.full((N_EP, EXPERTS * CAP), TOKB, jnp.int32)
    source = jax.vmap(lambda row, slot: row.at[slot].set(token_ids))(source, slots)
    padded = jnp.concatenate([normed.reshape(N_EP, TOKB, D), jnp.zeros((N_EP, 1, D), jnp.bfloat16)], axis=1)
    dispatched = jax.vmap(lambda rows, index: jnp.take(rows, index, axis=0))(padded, source)
    per_expert = jnp.transpose(dispatched.reshape(N_EP, EXPERTS, CAP, D), (1, 0, 2, 3)).reshape(EXPERTS, N_EP * CAP, D)
    outputs = lax.map(expert_apply, (per_expert, expert_gate_weight, expert_up_weight, expert_down_weight))
    by_source = jnp.transpose(outputs.reshape(EXPERTS, N_EP, CAP, D), (1, 0, 2, 3)).reshape(N_EP, EXPERTS * CAP, D)
    picked = jax.vmap(lambda rows, index: jnp.take(rows, index, axis=0))(by_source, slots).astype(jnp.float32)
    combined = lax.optimization_barrier(jnp.sum(picked.reshape(N_EP, TOKB, 2, D) * weights.reshape(N_EP, TOKB, 2, 1), axis=2))
    experts_out = combined.reshape(TOKENS, D).astype(jnp.bfloat16)
    return (mixer_out, experts_out)
```

```python
import functools
import math

import jax
import jax.numpy as jnp
from jax import lax
from jax.experimental import pallas as pl
from jax.experimental.pallas import tpu as pltpu
from jax.sharding import PartitionSpec as P

STATE = 64
GROUPS = 4
HEADS = 32
BLOCK = 128
CORES = 2
LANES = 128
HALO = 16
EPS = 1e-6
MESH = pl.DeviceIdType.MESH
F32 = jnp.float32
BF16 = jnp.bfloat16


def snake(i, n):
    w = math.isqrt(n)
    y, x = i // w, i % w
    odd = y % 2
    return y * w + x * (1 - 2 * odd) + odd * (w - 1)


def silu(v):
    return v / (1.0 + jnp.exp(-v))


def dot(a, b, dims=(((1,), (0,)), ((), ()))):
    return lax.dot_general(a, b, dims, preferred_element_type=F32)


def kernel(
    n_ep,
    n_tp,
    x_hbm,
    gate_hbm,
    b_hbm,
    c_hbm,
    wout_hbm,
    tok_hbm,
    eg_hbm,
    eu_hbm,
    ed_hbm,
    xtaps,
    btaps,
    ctaps,
    step,
    extra,
    lograte,
    dscale,
    gnorm,
    pnorm,
    router,
    routes,
    out,
    eout,
    xpad,
    bcpad,
    gate,
    eg,
    eu,
    ed,
    wk,
    rows_tok,
    wts,
    hid,
    psend,
    pmine,
    precv,
    rsrecv,
    zsend,
    zrecv,
    xs_s,
    bc_s,
    rows_s,
    prev_s,
    dpre_s,
    st_s,
    dec_s,
    smsg,
    srecv,
    ent,
    mixed,
    mrecv,
    pjsend,
    pjown,
    pjrecv,
    ld,
    halo_s,
    halo_r,
    tok_s,
    tok_r,
    tokp_s,
    tokp_r,
    wts_s,
    wts_r,
    wz_s,
    wz_r,
    wr_s,
    wr_r,
    state_s,
    state_r,
    pd_s,
    pd_r,
    rs_s,
    rs_r,
    zs_s,
    zs_r,
    a2a_s,
    a2a_r,
    pj_s,
    pj_r,
):
    n_z = n_tp // CORES
    half_ring = n_ep // 2
    e = lax.axis_index("ep")
    t = lax.axis_index("tp")
    c = t % CORES
    z = t // CORES
    ring = snake(e, n_ep)
    partner = (e, t + 1 - 2 * c)

    def at_ring(offset):
        return snake((ring + offset + n_ep) % n_ep, n_ep)

    next_ep, prev_ep = at_ring(1), at_ring(-1)
    toward = ((next_ep, t), (prev_ep, t))
    length, width = x_hbm.shape
    heads = width // STATE
    nblk = length // BLOCK
    group = t * heads // (HEADS // GROUPS)
    pair = group * STATE // LANES
    within = group * STATE % LANES
    n_tok, depth = tok_hbm.shape
    half = n_tok // CORES
    quarter = half // 2
    feats = depth // n_tp
    ff = eg_hbm.shape[1]
    rows_w = wout_hbm.shape[0]
    part = wout_hbm.shape[1] // n_ep
    rows_dev = out.shape[0]
    n_experts = n_ep
    pending = []

    def remote(src, dst, send, recv, device):
        return pltpu.make_async_remote_copy(
            src_ref=src, dst_ref=dst, send_sem=send, recv_sem=recv, device_id=device, device_id_type=MESH
        )

    def send(src, dst, send_sem, recv_sem, device):
        copy = remote(src, dst, send_sem, recv_sem, device)
        copy.start()
        pending.append(copy)
        return copy

    def arrived(view, sem):
        remote(view, view, sem, sem, partner).wait_recv()

    def local(src, dst, index):
        copy = pltpu.make_async_copy(src, dst, ld.at[index])
        copy.start()
        return copy

    get_tok = local(tok_hbm, rows_tok.at[e], 0)
    get_eg = local(eg_hbm, eg, 1)
    get_eu = local(eu_hbm, eu, 2)
    get_ed = local(ed_hbm, ed, 3)
    lane_b = pl.ds(pl.multiple_of(pair * LANES, LANES), LANES)
    get_x = local(x_hbm, xpad.at[pl.ds(HALO, length)], 4)
    get_b = local(b_hbm.at[:, lane_b], bcpad.at[pl.ds(HALO, length), pl.ds(0, LANES)], 5)
    get_c = local(c_hbm.at[:, lane_b], bcpad.at[pl.ds(HALO, length), pl.ds(LANES, LANES)], 6)
    get_gate = local(gate_hbm, gate, 7)
    get_w = [
        local(wout_hbm.at[:, pl.ds(q * part, part)], wk.at[q, z], 8 + q) for q in range(n_ep)
    ]

    barrier = pltpu.get_barrier_semaphore()
    peers = 0
    for k in range(1, n_ep):
        pl.semaphore_signal(barrier, inc=1, device_id=((e + k) % n_ep, t), device_id_type=MESH)
        peers += 1
    for k in range(1, n_z):
        pl.semaphore_signal(
            barrier, inc=1, device_id=(e, (t + CORES * k) % n_tp), device_id_type=MESH
        )
        peers += 1
    pl.semaphore_signal(barrier, inc=1, device_id=partner, device_id_type=MESH)
    peers += 1

    get_tok.wait()
    scale = pnorm[...].astype(F32)

    def norm_rows(i, carry):
        rows = pl.ds(pl.multiple_of(i * 32, 32), 32)
        v = rows_tok[e, rows, :].astype(F32)
        v = v * lax.rsqrt(jnp.mean(v * v, axis=-1, keepdims=True) + EPS) * scale
        rows_tok[e, rows, :] = v.astype(BF16)
        return carry

    lax.fori_loop(0, n_tok // 32, norm_rows, 0)

    pl.semaphore_wait(barrier, peers)

    def tok_rows(core, way, last):
        if last:
            return pl.ds(pl.multiple_of(core * half + way * quarter, quarter), quarter)
        return pl.ds(pl.multiple_of(core * half, half), half)

    def send_tokens(way, d):
        block = at_ring(-(d - 1) if way == 0 else d - 1)
        view = rows_tok.at[block, tok_rows(c, way, d == half_ring), :]
        send(view, view, tok_s.at[way, d - 1], tok_r.at[way, d - 1], toward[way])

    def share_tokens(way, d):
        block = at_ring(-d if way == 0 else d)
        view = rows_tok.at[block, tok_rows(c, way, d == half_ring), :]
        arrived(view, tok_r.at[way, d - 1])
        if d < half_ring:
            send_tokens(way, d + 1)
        send(view, view, tokp_s.at[way, d - 1], tokp_r.at[way, d - 1], partner)

    def shared_tokens(way, d):
        block = at_ring(-d if way == 0 else d)
        view = rows_tok.at[block, tok_rows(1 - c, way, d == half_ring), :]
        arrived(view, tokp_r.at[way, d - 1])

    for way in range(2):
        send_tokens(way, 1)

    tail_rows = pl.ds(length - HALO, HALO)
    head_rows = pl.ds(0, HALO)
    halo = [
        remote(src, dst, halo_s.at[i], halo_r.at[i], ((e + 1) % n_ep, t))
        for i, (src, dst) in enumerate(
            (
                (x_hbm.at[tail_rows], xpad.at[head_rows]),
                (b_hbm.at[tail_rows, lane_b], bcpad.at[head_rows, pl.ds(0, LANES)]),
                (c_hbm.at[tail_rows, lane_b], bcpad.at[head_rows, pl.ds(LANES, LANES)]),
            )
        )
    ]

    @pl.when(e < n_ep - 1)
    def _():
        for copy in halo:
            copy.start()

    @pl.when(e == 0)
    def _():
        xpad[head_rows, :] = jnp.zeros((HALO, width), BF16)
        bcpad[head_rows, :] = jnp.zeros((HALO, 2 * LANES), BF16)

    mine = pl.ds(pl.multiple_of(e * part, part), part)
    for k in range(1, n_z):
        send(
            wout_hbm.at[:, mine],
            wk.at[e, z],
            wz_s.at[k - 1],
            wz_r.at[k - 1],
            (e, (t + CORES * k) % n_tp),
        )

    logits = dot(router[...], rows_tok[e], (((1,), (1,)), ((), ())))
    expert_logit = [logits[i : i + 1, :] for i in range(n_experts)]
    n_grp = max(1, n_experts // 4)
    per_group = n_experts // n_grp
    group_logit = [logits[n_experts + i : n_experts + i + 1, :] for i in range(n_grp)]

    def log_softmax(rows):
        top = functools.reduce(jnp.maximum, rows)
        norm = jnp.log(functools.reduce(jnp.add, [jnp.exp(v - top) for v in rows]))
        return [v - top - norm for v in rows]

    group_lp = log_softmax(group_logit)
    total_lp = []
    for i in range(n_grp):
        inner = log_softmax(expert_logit[i * per_group : (i + 1) * per_group])
        total_lp += [group_lp[i] + v for v in inner]
    picks = [routes[k : k + 1, :] for k in range(2)]
    chosen = []
    for k in range(2):
        value = jnp.zeros_like(total_lp[0])
        for i in range(n_experts):
            value = jnp.where(picks[k] == i, total_lp[i], value)
        chosen.append(value)
    top = jnp.maximum(chosen[0], chosen[1])
    share = [jnp.exp(v - top) for v in chosen]
    inv = 1.0 / (share[0] + share[1])
    share = [v * inv for v in share]
    wts[e] = jnp.zeros(wts.shape[1:], F32)
    for i in range(n_experts):
        wts[e, i : i + 1, :] = jnp.where(picks[0] == i, share[0], 0.0) + jnp.where(
            picks[1] == i, share[1], 0.0
        )
    for k in range(1, n_ep):
        send(wts.at[e], wts.at[e], wts_s.at[k - 1], wts_r.at[k - 1], ((e + k) % n_ep, t))

    slots = psend.shape[0]
    to_partner = {}

    def experts(block, order):
        wrow = wts[block, pl.ds(e, 1), :]
        wcol = jnp.transpose(jnp.broadcast_to(wrow, (LANES, n_tok)))
        wide = 256
        wcol = jnp.concatenate([wcol] * (wide // LANES), axis=1)

        def up(j, carry):
            cols = pl.ds(pl.multiple_of(j * wide, wide), wide)
            g = dot(rows_tok[block], eg[:, cols])
            u = dot(rows_tok[block], eu[:, cols])
            hid[:, cols] = (silu(g) * u * wcol).astype(BF16)
            return carry

        lax.fori_loop(0, ff // wide, up, 0)
        slot = order % slots
        if order >= slots:
            earlier = to_partner[order - slots]
            earlier.wait_send()
            pending[:] = [copy for copy in pending if copy is not earlier]

        def down(k, carry):
            at = pl.ds(pl.multiple_of(k * feats, feats), feats)
            other = pl.ds(pl.multiple_of((CORES * k + 1 - c) * feats, feats), feats)
            own = pl.ds(pl.multiple_of((CORES * k + c) * feats, feats), feats)
            psend[slot, :, at] = dot(hid[...], ed[:, other]).astype(BF16)
            pmine[block, :, at] = dot(hid[...], ed[:, own]).astype(BF16)
            return carry

        lax.fori_loop(0, n_z, down, 0)
        to_partner[order] = send(
            psend.at[slot], precv.at[block], pd_s.at[order], pd_r.at[order], partner
        )

    get_eg.wait()
    get_eu.wait()
    get_ed.wait()
    experts(e, 0)

    lane = lax.broadcasted_iota(jnp.int32, (1, LANES), 1)
    rate = jnp.exp(lograte[...])
    for k in range(nblk):
        at = pl.ds(k * BLOCK, BLOCK)
        v = step[:, at]
        dt = jnp.maximum(v, 0.0) + jnp.log(1.0 + jnp.exp(-jnp.abs(v)))
        cum = extra[:, at] - dt * rate
        hop = 1
        while hop < BLOCK:
            cum = cum + jnp.where(lane >= hop, pltpu.roll(cum, hop, 1), 0.0)
            hop *= 2
        grown = jnp.exp(cum)
        left = jnp.exp(cum[:, BLOCK - 1 :] - cum) * dt
        rows_s[k, 0:heads, :] = cum
        rows_s[k, 8 : 8 + heads, :] = dt
        rows_s[k, 16 : 16 + heads, :] = left
        rows_s[k, 24 : 24 + heads, :] = grown

    def spread(cols, first):
        pieces = []
        for j in range(width // LANES):
            low = cols[:, first + 2 * j : first + 2 * j + 1]
            high = cols[:, first + 2 * j + 1 : first + 2 * j + 2]
            pieces.append(jnp.where(lane < STATE, low, high))
        return jnp.concatenate(pieces, axis=1) if len(pieces) > 1 else pieces[0]

    get_x.wait()
    get_b.wait()
    get_c.wait()

    @pl.when(e > 0)
    def _():
        for copy in halo:
            copy.wait_recv()

    x_w = xtaps[...].astype(F32)
    bc_w = jnp.concatenate([btaps[:, lane_b], ctaps[:, lane_b]], axis=1).astype(F32)
    lane2 = lax.broadcasted_iota(jnp.int32, (1, 2 * LANES), 1) % LANES
    in_group = (lane2 >= within) & (lane2 < within + STATE)
    taps = x_w.shape[0]

    def conv(ref, w, k):
        v = ref[pl.ds(pl.multiple_of(k * BLOCK, BLOCK), BLOCK + HALO), :].astype(F32)
        total = v[HALO:] * w[taps - 1 :]
        for j in range(taps - 1):
            total = total + pltpu.roll(v, taps - 1 - j, 0)[HALO:] * w[j : j + 1]
        return silu(total)

    st_s[...] = jnp.zeros_like(st_s)
    dec_s[...] = jnp.ones_like(dec_s)

    def first_pass(k, carry):
        rows = pl.ds(pl.multiple_of(k * BLOCK, BLOCK), BLOCK)
        xs = conv(xpad, x_w, k).astype(BF16)
        bc = jnp.where(in_group, conv(bcpad, bc_w, k), 0.0).astype(BF16)
        xs_s[rows, :] = xs
        bc_s[rows, :] = bc
        cols = jnp.transpose(rows_s[k])
        xw = (xs.astype(F32) * spread(cols, 16)).astype(BF16)
        block_state = dot(bc[:, :LANES], xw, (((0,), (0,)), ((), ())))
        gone = spread(cols[BLOCK - 8 :, :], 24)[7:8, :]
        prev_s[k] = st_s[...]
        dpre_s[k] = dec_s[...]
        st_s[...] = st_s[...] * gone + block_state
        dec_s[...] = dec_s[...] * gone
        return carry

    lax.fori_loop(0, nblk, first_pass, 0)

    group_rows = pl.ds(pl.multiple_of(within, STATE), STATE)
    smsg[0:STATE, :] = st_s[group_rows, :].astype(BF16)
    smsg[STATE : STATE + 16, :] = jnp.concatenate([dec_s[...]] * 2, axis=0).astype(BF16)
    state_copies = [
        remote(smsg, srecv.at[k], state_s.at[k], state_r.at[k], ((e + 1 + k) % n_ep, t))
        for k in range(n_ep - 1)
    ]
    for k, copy in enumerate(state_copies):
        pl.when(e + 1 + k < n_ep)(copy.start)

    for k in range(1, n_ep):
        src = (e - k + n_ep) % n_ep
        arrived(wts.at[src], wts_r.at[k - 1])
    for d in range(1, half_ring + 1):
        for way in range(2):
            share_tokens(way, d)
        if d == 1:
            for k in range(1, n_z):
                arrived(wk.at[e, (z - k + n_z) % n_z], wz_r.at[k - 1])

            def weight_view(block, way, k, last):
                slab = wk.at[block, (z - k + n_z) % n_z]
                if last:
                    return slab.at[pl.ds(way * (rows_w // 2), rows_w // 2), :]
                return slab

            def send_weight(way, step_d):
                block = at_ring(-(step_d - 1) if way == 0 else step_d - 1)
                for k in range(1, n_z):
                    view = weight_view(block, way, k, step_d == half_ring)
                    send(
                        view,
                        view,
                        wr_s.at[way, step_d - 1, k - 1],
                        wr_r.at[way, step_d - 1, k - 1],
                        toward[way],
                    )

            def weight_arrived(way, step_d):
                block = at_ring(-step_d if way == 0 else step_d)
                for k in range(1, n_z):
                    view = weight_view(block, way, k, step_d == half_ring)
                    arrived(view, wr_r.at[way, step_d - 1, k - 1])

            for way in range(2):
                send_weight(way, 1)
        for way in range(2):
            shared_tokens(way, d)
        if d < half_ring:
            for way in range(2):
                order = 2 * d - 1 + way
                experts(at_ring(-d if way == 0 else d), order)
        else:
            order = 2 * d - 1
            experts(at_ring(d), order)

    def order_of(way, d):
        if d == half_ring:
            return 2 * d - 1
        if d == 0:
            return 0
        return 2 * d - 1 + way

    def partner_sum(block, order):
        arrived(precv.at[block], pd_r.at[order])

    keep = feats * n_z
    keep_half = keep // 2

    def ring_sum(d, way):
        block = at_ring(d if way == 0 else -d)
        if d == half_ring:
            cols = pl.ds(way * keep_half, keep_half)
            value = pmine[block, :, cols].astype(F32) + precv[block, :, cols].astype(F32)
            pmine[block, :, cols] = value.astype(BF16)
            view = pmine.at[block, :, cols]
            send(
                view, rsrecv.at[way, d - 1, :, cols], rs_s.at[way, d - 1], rs_r.at[way, d - 1], toward[way]
            )
            return
        last = d == half_ring - 1
        cols = pl.ds(way * keep_half, keep_half) if last else pl.ds(0, keep)
        arrived(rsrecv.at[way, d, :, cols], rs_r.at[way, d])
        if last:
            rest = pl.ds((1 - way) * keep_half, keep_half)
            pmine[block, :, rest] = (
                pmine[block, :, rest].astype(F32) + precv[block, :, rest].astype(F32)
            ).astype(BF16)
        pmine[block, :, cols] = (
            pmine[block, :, cols].astype(F32)
            + precv[block, :, cols].astype(F32)
            + rsrecv[way, d, :, cols].astype(F32)
        ).astype(BF16)
        send(
            pmine.at[block], rsrecv.at[way, d - 1], rs_s.at[way, d - 1], rs_r.at[way, d - 1], toward[way]
        )

    partner_sum(at_ring(half_ring), order_of(0, half_ring))
    for way in range(2):
        ring_sum(half_ring, way)

    ent[...] = jnp.zeros_like(ent)
    for k in reversed(range(n_ep - 1)):

        @pl.when(e > k)
        def _(k=k):
            arrived(srecv.at[k], state_r.at[k])
            before = ent[group_rows, :]
            gone = srecv[k, STATE : STATE + 16, :].astype(F32)[0:1, :]
            ent[group_rows, :] = before * gone + srecv[k, 0:STATE, :].astype(F32)

    get_gate.wait()
    d_row = dscale[...]
    g_row = gnorm[...].astype(F32)
    row_id = lax.broadcasted_iota(jnp.int32, (BLOCK, BLOCK), 0)
    col_id = lax.broadcasted_iota(jnp.int32, (BLOCK, BLOCK), 1)
    same_head = (
        lax.broadcasted_iota(jnp.int32, (width, width), 0) // STATE
        == lax.broadcasted_iota(jnp.int32, (width, width), 1) // STATE
    )
    mean_of = jnp.where(same_head, 1.0 / STATE, 0.0).astype(BF16)

    def second_pass(k):
        rows = pl.ds(pl.multiple_of(k * BLOCK, BLOCK), BLOCK)
        xs_f = xs_s[rows, :].astype(F32)
        bs = bc_s[rows, pl.ds(0, LANES)]
        cs = bc_s[rows, pl.ds(LANES, LANES)]
        row_q = rows_s[k]
        cols = jnp.transpose(row_q)
        scores = dot(cs, bs, (((1,), (1,)), ((), ())))
        x_dt = (xs_f * spread(cols, 8)).astype(BF16)
        inner = []
        for j in range(width // LANES):
            both = []
            for h in (2 * j, 2 * j + 1):
                diff = cols[:, h : h + 1] - row_q[h : h + 1, :]
                link = jnp.exp(jnp.where(row_id >= col_id, diff, -1e30))
                both.append(dot((scores * link).astype(BF16), x_dt[:, j * LANES : (j + 1) * LANES]))
            inner.append(jnp.where(lane < STATE, both[0], both[1]))
        inner = jnp.concatenate(inner, axis=1) if len(inner) > 1 else inner[0]
        prev = prev_s[k] + ent[...] * dpre_s[k, 0:1, :]
        carried = dot(cs, prev.astype(BF16)) * spread(cols, 24)
        gated = (inner + carried + d_row * xs_f) * silu(gate[rows, :].astype(F32))
        square = gated * gated
        high = square.astype(BF16)
        low = (square - high.astype(F32)).astype(BF16)
        mean = dot(high, mean_of) + dot(low, mean_of)
        mixed[rows, :] = (gated * lax.rsqrt(mean + EPS) * g_row).astype(BF16)

    chip_rows = rows_dev * CORES
    per_chip = chip_rows // BLOCK

    def mix_for(k):
        target = (z + k) % n_z

        def body(i, carry):
            second_pass(target * per_chip + i)
            return carry

        lax.fori_loop(0, per_chip, body, 0)
        view = mixed.at[pl.ds(pl.multiple_of(target * chip_rows, chip_rows), chip_rows), :]
        if k:
            send(view, mrecv.at[z], a2a_s.at[k - 1], a2a_r.at[k - 1], (e, (t + CORES * k) % n_tp))
        else:
            own = pl.ds(pl.multiple_of(z * chip_rows, chip_rows), chip_rows)
            mrecv[z] = mixed[own, :]

    def ring_step(d):
        for way in range(2):
            partner_sum(at_ring(d if way == 0 else -d), order_of(1 - way, d))
            ring_sum(d, way)

    ring_steps = list(range(half_ring - 1, 0, -1))
    weight_steps = list(range(1, half_ring + 1))
    for i, k in enumerate(list(range(1, n_z)) + [0]):
        mix_for(k)
        if i >= n_z // 2 - 1 and ring_steps:
            ring_step(ring_steps.pop(0))
        if i >= n_z // 2 and weight_steps and weight_steps[0] < half_ring:
            d = weight_steps.pop(0)
            for way in range(2):
                weight_arrived(way, d)
                send_weight(way, d + 1)
    for d in ring_steps:
        ring_step(d)

    partner_sum(e, 0)
    for way in range(2):
        arrived(rsrecv.at[way, 0], rs_r.at[way, 0])

    def own_sum(target):
        at = pl.ds(pl.multiple_of(target * feats, feats), feats)
        return (
            pmine[e, :, at].astype(F32)
            + precv[e, :, at].astype(F32)
            + rsrecv[0, 0, :, at].astype(F32)
            + rsrecv[1, 0, :, at].astype(F32)
        )

    for k in range(1, n_z):
        target = (z + k) % n_z
        zsend[k - 1] = own_sum(target).astype(BF16)
        send(zsend.at[k - 1], zrecv.at[k - 1], zs_s.at[k - 1], zs_r.at[k - 1], (e, (t + CORES * k) % n_tp))

    while weight_steps and weight_steps[0] < half_ring:
        d = weight_steps.pop(0)
        for way in range(2):
            weight_arrived(way, d)
            send_weight(way, d + 1)

    for k in range(1, n_z):
        arrived(mrecv.at[(z - k + n_z) % n_z], a2a_r.at[k - 1])
    for copy in get_w:
        copy.wait()

    def project(block, order):
        def rows_of(core):
            return pl.ds(pl.multiple_of(core * rows_dev, rows_dev), rows_dev)

        def product(core):
            total = dot(mrecv[0, rows_of(core), :], wk[block, 0])
            for k in range(1, n_z):
                total = total + dot(mrecv[k, rows_of(core), :], wk[block, k])
            return total

        pjsend[order] = product(1 - c)
        send(pjsend.at[order], pjrecv.at[order], pj_s.at[order], pj_r.at[order], partner)
        pjown[order] = product(c)

    def finish(block, order):
        arrived(pjrecv.at[order], pj_r.at[order])
        cols = pl.ds(pl.multiple_of(block * part, part), part)
        out[:, cols] = (pjown[order] + pjrecv[order]).astype(BF16)

    project(e, 0)
    done = [(e, 0)]
    for d in range(1, half_ring):
        for way in range(2):
            block = at_ring(-d if way == 0 else d)
            project(block, order_of(way, d))
            done.append((block, order_of(way, d)))

    total = own_sum(z)
    for k in range(1, n_z):
        arrived(zrecv.at[k - 1], zs_r.at[k - 1])
        total = total + zrecv[k - 1].astype(F32)
    eout[...] = total.astype(BF16)

    for way in range(2):
        weight_arrived(way, half_ring)
    block = at_ring(half_ring)
    project(block, order_of(0, half_ring))
    done.append((block, order_of(0, half_ring)))
    for block, order in done:
        finish(block, order)

    for copy in pending:
        copy.wait_send()

    @pl.when(e < n_ep - 1)
    def _():
        for copy in halo:
            copy.wait_send()

    for k, copy in enumerate(state_copies):
        pl.when(e + 1 + k < n_ep)(copy.wait_send)


def fused(n_ep, n_tp, args):
    (
        x,
        gate_logits,
        b_map,
        c_map,
        xtaps,
        btaps,
        ctaps,
        step,
        lograte,
        extra,
        dscale,
        gnorm,
        wout,
        tokens,
        pnorm,
        group_cols,
        expert_cols,
        routes,
        eg,
        eu,
        ed,
    ) = args
    n_z = n_tp // CORES
    half_ring = n_ep // 2
    length, width = x.shape
    heads = dscale.shape[0]
    nblk = length // BLOCK
    n_tok, depth = tokens.shape
    feats = depth // n_tp
    ff = eg.shape[2]
    rows_w, cols_w = wout.shape
    part = cols_w // n_ep
    rows_dev = length // n_tp
    chip_rows = rows_dev * CORES
    n_rows = expert_cols.shape[1] + group_cols.shape[1]
    router = jnp.concatenate([expert_cols, group_cols], axis=1).T
    router = jnp.pad(router, ((0, -n_rows % 16), (0, 0)))
    w_rows = -(-expert_cols.shape[1] // 8) * 8
    slots = max(2, min(n_ep, 16 // n_ep))
    keep = n_z * feats
    anywhere = pl.BlockSpec(memory_space=pl.ANY)
    vmem = pl.BlockSpec(memory_space=pltpu.VMEM)
    dma = pltpu.SemaphoreType.DMA
    scratch = [
        pltpu.VMEM((length + HALO, width), BF16),
        pltpu.VMEM((length + HALO, 2 * LANES), BF16),
        pltpu.VMEM((length, width), BF16),
        pltpu.VMEM((depth, ff), BF16),
        pltpu.VMEM((depth, ff), BF16),
        pltpu.VMEM((ff, depth), BF16),
        pltpu.VMEM((n_ep, n_z, rows_w, part), BF16),
        pltpu.VMEM((n_ep, n_tok, depth), BF16),
        pltpu.VMEM((n_ep, w_rows, n_tok), F32),
        pltpu.VMEM((n_tok, ff), BF16),
        pltpu.VMEM((slots, n_tok, keep), BF16),
        pltpu.VMEM((n_ep, n_tok, keep), BF16),
        pltpu.VMEM((n_ep, n_tok, keep), BF16),
        pltpu.VMEM((2, half_ring, n_tok, keep), BF16),
        pltpu.VMEM((n_z - 1, n_tok, feats), BF16),
        pltpu.VMEM((n_z - 1, n_tok, feats), BF16),
        pltpu.VMEM((length, width), BF16),
        pltpu.VMEM((length, 2 * LANES), BF16),
        pltpu.VMEM((nblk, BLOCK, BLOCK), F32),
        pltpu.VMEM((nblk, LANES, width), F32),
        pltpu.VMEM((nblk, 8, width), F32),
        pltpu.VMEM((LANES, width), F32),
        pltpu.VMEM((8, width), F32),
        pltpu.VMEM((STATE + 16, width), BF16),
        pltpu.VMEM((n_ep - 1, STATE + 16, width), BF16),
        pltpu.VMEM((LANES, width), F32),
        pltpu.VMEM((length, width), BF16),
        pltpu.VMEM((n_z, chip_rows, width), BF16),
        pltpu.VMEM((n_ep, rows_dev, part), F32),
        pltpu.VMEM((n_ep, rows_dev, part), F32),
        pltpu.VMEM((n_ep, rows_dev, part), F32),
        dma((8 + n_ep,)),
        dma((3,)),
        dma((3,)),
    ]
    for shape in (
        (2, half_ring),
        (2, half_ring),
        (n_ep - 1,),
        (n_z - 1,),
        (2, half_ring, n_z - 1),
        (n_ep - 1,),
        (n_ep,),
        (2, half_ring),
        (n_z - 1,),
        (n_z - 1,),
        (n_ep,),
    ):
        scratch += [dma(shape), dma(shape)]
    return pl.pallas_call(
        functools.partial(kernel, n_ep, n_tp),
        out_shape=(
            jax.ShapeDtypeStruct((rows_dev, cols_w), BF16),
            jax.ShapeDtypeStruct((n_tok, feats), BF16),
        ),
        in_specs=[anywhere] * 9 + [vmem] * 11,
        out_specs=(vmem, vmem),
        scratch_shapes=scratch,
        name="fused",
        compiler_params=pltpu.CompilerParams(
            collective_id=0, has_side_effects=True, vmem_limit_bytes=67_000_000
        ),
    )(
        x,
        gate_logits,
        b_map,
        c_map,
        wout,
        tokens,
        eg[0],
        eu[0],
        ed[0],
        xtaps,
        btaps,
        ctaps,
        step,
        extra,
        lograte.reshape(heads, 1),
        jnp.repeat(dscale, width // heads).reshape(1, width),
        gnorm.reshape(1, width),
        pnorm.reshape(1, depth),
        router,
        routes.T,
    )


def solution(mesh):
    n_ep, n_tp = mesh.shape["ep"], mesh.shape["tp"]
    in_specs = (
        P("ep", "tp"),
        P("ep", "tp"),
        P("ep", None),
        P("ep", None),
        P(None, "tp"),
        P(),
        P(),
        P("tp", "ep"),
        P("tp"),
        P("tp", "ep"),
        P("tp"),
        P("tp"),
        P("tp", None),
        P("ep", None),
        P(),
        P(),
        P(),
        P("ep", None),
        P("ep", None, "tp"),
        P("ep", None, "tp"),
        P("ep", "tp", None),
    )
    out_specs = (P(("ep", "tp"), None), P("ep", "tp"))
    return jax.shard_map(
        lambda *args: fused(n_ep, n_tp, args),
        mesh=mesh,
        in_specs=in_specs,
        out_specs=out_specs,
        check_vma=False,
    )
```

```python
import functools
import math

import jax
import jax.numpy as jnp
from jax import lax
from jax.experimental import pallas as pl
from jax.experimental.pallas import tpu as pltpu
from jax.sharding import PartitionSpec as P

STATE = 64
GROUPS = 4
HEADS = 32
BLOCK = 128
CORES = 2
LANES = 128
HALO = 16
EPS = 1e-6
MESH = pl.DeviceIdType.MESH
F32 = jnp.float32
BF16 = jnp.bfloat16


def snake(i, n):
    w = math.isqrt(n)
    y, x = i // w, i % w
    odd = y % 2
    return y * w + x * (1 - 2 * odd) + odd * (w - 1)


def silu(v):
    return v / (1.0 + jnp.exp(-v))


def dot(a, b, dims=(((1,), (0,)), ((), ()))):
    return lax.dot_general(a, b, dims, preferred_element_type=F32)


def kernel(
    n_ep,
    n_tp,
    x_hbm,
    gate_hbm,
    b_hbm,
    c_hbm,
    wout_hbm,
    tok_hbm,
    eg_hbm,
    eu_hbm,
    ed_hbm,
    xtaps,
    btaps,
    ctaps,
    step,
    extra,
    lograte,
    dscale,
    gnorm,
    pnorm,
    grouter,
    erouter,
    routes,
    out,
    eout,
    xpad,
    bcpad,
    gate,
    eg,
    eu,
    ed,
    wk,
    rows_tok,
    wts,
    hid,
    psend,
    pmine,
    precv,
    rsrecv,
    zsend,
    zrecv,
    xs_s,
    bc_s,
    rows_s,
    prev_s,
    dpre_s,
    st_s,
    dec_s,
    smsg,
    srecv,
    ent,
    mixed,
    mrecv,
    pjsend,
    pjown,
    pjlast,
    pjrecv,
    result,
    eresult,
    ld,
    halo_s,
    halo_r,
    tok_s,
    tok_r,
    tokp_s,
    tokp_r,
    wts_s,
    wts_r,
    wz_s,
    wz_r,
    wr_s,
    wr_r,
    state_s,
    state_r,
    pd_s,
    pd_r,
    rs_s,
    rs_r,
    zs_s,
    zs_r,
    a2a_s,
    a2a_r,
    pj_s,
    pj_r,
):
    n_z = n_tp // CORES
    half_ring = n_ep // 2
    e = lax.axis_index("ep")
    t = lax.axis_index("tp")
    c = t % CORES
    z = t // CORES
    ring = snake(e, n_ep)
    partner = (e, t + 1 - 2 * c)

    def across_z(k):
        place, bit = 0, 1
        while bit < n_z:
            own = z // bit % 2
            place = place + bit * ((1 - own) if k & bit else own)
            bit *= 2
        return place

    def z_device(k):
        return (e, CORES * across_z(k) + c)

    def at_ring(offset):
        return snake((ring + offset + n_ep) % n_ep, n_ep)

    next_ep, prev_ep = at_ring(1), at_ring(-1)
    toward = ((next_ep, t), (prev_ep, t))
    length, width = x_hbm.shape
    heads = width // STATE
    nblk = length // BLOCK
    group = t * heads // (HEADS // GROUPS)
    pair = group * STATE // LANES
    within = group * STATE % LANES
    n_tok, depth = tok_hbm.shape
    half = n_tok // CORES
    quarter = half // 2
    feats = depth // n_tp
    ff = eg_hbm.shape[1]
    rows_w = wout_hbm.shape[0]
    part = wout_hbm.shape[1] // n_ep
    rows_dev = out.shape[0]
    pending = []

    def remote(src, dst, send, recv, device):
        return pltpu.make_async_remote_copy(
            src_ref=src, dst_ref=dst, send_sem=send, recv_sem=recv, device_id=device, device_id_type=MESH
        )

    def send(src, dst, send_sem, recv_sem, device):
        copy = remote(src, dst, send_sem, recv_sem, device)
        copy.start()
        pending.append(copy)
        return copy

    def arrived(view, sem):
        remote(view, view, sem, sem, partner).wait_recv()

    def local(src, dst, index):
        copy = pltpu.make_async_copy(src, dst, ld.at[index])
        copy.start()
        return copy

    get_tok = local(tok_hbm, rows_tok.at[e], 0)
    get_eg = local(eg_hbm, eg, 1)
    get_eu = local(eu_hbm, eu, 2)
    get_ed = local(ed_hbm, ed, 3)
    lane_b = pl.ds(pl.multiple_of(pair * LANES, LANES), LANES)
    get_x = local(x_hbm, xpad.at[pl.ds(HALO, length)], 4)
    get_b = local(b_hbm.at[:, lane_b], bcpad.at[pl.ds(HALO, length), pl.ds(0, LANES)], 5)
    get_c = local(c_hbm.at[:, lane_b], bcpad.at[pl.ds(HALO, length), pl.ds(LANES, LANES)], 6)
    get_gate = local(gate_hbm, gate, 7)
    get_w = [
        local(wout_hbm.at[:, pl.ds(q * part, part)], wk.at[q, z], 8 + q) for q in range(n_ep)
    ]

    barrier = pltpu.get_barrier_semaphore()
    peers = 0
    for k in range(1, n_ep):
        pl.semaphore_signal(barrier, inc=1, device_id=((e + k) % n_ep, t), device_id_type=MESH)
        peers += 1
    for k in range(1, n_z):
        pl.semaphore_signal(barrier, inc=1, device_id=z_device(k), device_id_type=MESH)
        peers += 1
    pl.semaphore_signal(barrier, inc=1, device_id=partner, device_id_type=MESH)
    peers += 1

    get_tok.wait()
    scale = pnorm[...].astype(F32).reshape(1, depth)

    def norm_rows(i, carry):
        rows = pl.ds(pl.multiple_of(i * 32, 32), 32)
        v = rows_tok[e, rows, :].astype(F32)
        v = v * lax.rsqrt(jnp.mean(v * v, axis=-1, keepdims=True) + EPS) * scale
        rows_tok[e, rows, :] = v.astype(BF16)
        return carry

    lax.fori_loop(0, n_tok // 32, norm_rows, 0)

    pl.semaphore_wait(barrier, peers)

    def tok_view(core, way, d, piece):
        block = at_ring(-d if way == 0 else d)
        if piece == 0:
            first, count = core * half + way * quarter, quarter
        else:
            count = quarter // 2
            first = core * half + (1 - way) * quarter + (piece - 1) * count
        return rows_tok.at[block, pl.ds(pl.multiple_of(first, count), count), :]

    def pieces_of(d):
        return range(1 if d == half_ring else 3)

    def send_tokens(way, d, piece):
        view = tok_view(c, way, d - 1, piece)
        send(view, view, tok_s.at[way, d - 1, piece], tok_r.at[way, d - 1, piece], toward[way])

    def share_tokens(d, pieces):
        for piece in pieces:
            for way in range(2):
                view = tok_view(c, way, d, piece)
                arrived(view, tok_r.at[way, d - 1, piece])
                if d < half_ring and piece in pieces_of(d + 1):
                    send_tokens(way, d + 1, piece)
                send(view, view, tokp_s.at[way, d - 1, piece], tokp_r.at[way, d - 1, piece], partner)

    def shared_tokens(way, d):
        for piece in pieces_of(d):
            arrived(tok_view(1 - c, way, d, piece), tokp_r.at[way, d - 1, piece])

    tail_rows = pl.ds(length - HALO, HALO)
    head_rows = pl.ds(0, HALO)
    halo = [
        remote(src, dst, halo_s.at[i], halo_r.at[i], ((e + 1) % n_ep, t))
        for i, (src, dst) in enumerate(
            (
                (x_hbm.at[tail_rows], xpad.at[head_rows]),
                (b_hbm.at[tail_rows, lane_b], bcpad.at[head_rows, pl.ds(0, LANES)]),
                (c_hbm.at[tail_rows, lane_b], bcpad.at[head_rows, pl.ds(LANES, LANES)]),
            )
        )
    ]

    @pl.when(e < n_ep - 1)
    def _():
        for copy in halo:
            copy.start()

    @pl.when(e == 0)
    def _():
        xpad[head_rows, :] = jnp.zeros((HALO, width), BF16)
        bcpad[head_rows, :] = jnp.zeros((HALO, 2 * LANES), BF16)

    for piece in range(2):
        for way in range(2):
            send_tokens(way, 1, piece)

    mine = pl.ds(pl.multiple_of(e * part, part), part)
    z_order = sorted(range(1, n_z), key=lambda k: (k != 1, -k))
    for k in z_order:
        send(
            wout_hbm.at[:, mine],
            wk.at[e, z],
            wz_s.at[k - 1],
            wz_r.at[k - 1],
            z_device(k),
        )

    n_experts, n_grp = erouter.shape[0], grouter.shape[0]
    over_rows = (((1,), (1,)), ((), ()))
    logits = dot(erouter[...], rows_tok[e], over_rows)
    expert_logit = [logits[i : i + 1, :] for i in range(n_experts)]
    logits = dot(grouter[...], rows_tok[e], over_rows)
    per_group = n_experts // n_grp
    group_logit = [logits[i : i + 1, :] for i in range(n_grp)]

    def log_softmax(rows):
        top = functools.reduce(jnp.maximum, rows)
        norm = jnp.log(functools.reduce(jnp.add, [jnp.exp(v - top) for v in rows]))
        return [v - top - norm for v in rows]

    group_lp = log_softmax(group_logit)
    total_lp = []
    for i in range(n_grp):
        inner = log_softmax(expert_logit[i * per_group : (i + 1) * per_group])
        total_lp += [group_lp[i] + v for v in inner]
    picks = [routes[k : k + 1, :] for k in range(2)]
    chosen = []
    for k in range(2):
        value = jnp.zeros_like(total_lp[0])
        for i in range(n_experts):
            value = jnp.where(picks[k] == i, total_lp[i], value)
        chosen.append(value)
    top = jnp.maximum(chosen[0], chosen[1])
    share = [jnp.exp(v - top) for v in chosen]
    inv = 1.0 / (share[0] + share[1])
    share = [v * inv for v in share]
    wts[e] = jnp.zeros(wts.shape[1:], F32)
    for i in range(n_experts):
        wts[e, i : i + 1, :] = jnp.where(picks[0] == i, share[0], 0.0) + jnp.where(
            picks[1] == i, share[1], 0.0
        )
    for k in range(1, n_ep):
        send(wts.at[e], wts.at[e], wts_s.at[k - 1], wts_r.at[k - 1], ((e + k) % n_ep, t))

    slots = psend.shape[0]
    to_partner = {}

    def experts(block, order):
        wrow = wts[block, pl.ds(e, 1), :]
        wcol = jnp.transpose(jnp.broadcast_to(wrow, (LANES, n_tok)))
        wide = 256
        wcol = jnp.concatenate([wcol] * (wide // LANES), axis=1)

        def up(j, carry):
            cols = pl.ds(pl.multiple_of(j * wide, wide), wide)
            g = dot(rows_tok[block], eg[:, cols])
            u = dot(rows_tok[block], eu[:, cols])
            hid[:, cols] = (silu(g) * u * wcol).astype(BF16)
            return carry

        lax.fori_loop(0, ff // wide, up, 0)
        slot = order % slots
        if order >= slots:
            earlier = to_partner[order - slots]
            earlier.wait_send()
            pending[:] = [copy for copy in pending if copy is not earlier]

        def down(into, core):
            for k in range(n_z):
                at = pl.ds(k * feats, feats)
                cols = pl.ds(pl.multiple_of((CORES * k + core) * feats, feats), feats)
                into[:, at] = dot(hid[...], ed[:, cols]).astype(BF16)

        down(psend.at[slot], 1 - c)
        to_partner[order] = send(
            psend.at[slot], precv.at[block], pd_s.at[order], pd_r.at[order], partner
        )
        down(pmine.at[block], c)

    lane = lax.broadcasted_iota(jnp.int32, (1, LANES), 1)
    head_row = lax.broadcasted_iota(jnp.int32, (heads, 1), 0)
    rate = jnp.zeros((heads, 1), F32)
    for h in range(heads):
        rate = jnp.where(head_row == h, lograte[h], rate)
    rate = jnp.exp(rate)
    for k in range(nblk):
        at = pl.ds(k * BLOCK, BLOCK)
        v = step[:, at]
        dt = jnp.maximum(v, 0.0) + jnp.log(1.0 + jnp.exp(-jnp.abs(v)))
        cum = extra[:, at] - dt * rate
        hop = 1
        while hop < BLOCK:
            cum = cum + jnp.where(lane >= hop, pltpu.roll(cum, hop, 1), 0.0)
            hop *= 2
        grown = jnp.exp(cum)
        left = jnp.exp(cum[:, BLOCK - 1 :] - cum) * dt
        rows_s[k, 0:heads, :] = cum
        rows_s[k, 8 : 8 + heads, :] = dt
        rows_s[k, 16 : 16 + heads, :] = left
        rows_s[k, 24 : 24 + heads, :] = grown

    def spread(cols, first):
        pieces = []
        for j in range(width // LANES):
            low = cols[:, first + 2 * j : first + 2 * j + 1]
            high = cols[:, first + 2 * j + 1 : first + 2 * j + 2]
            pieces.append(jnp.where(lane < STATE, low, high))
        return jnp.concatenate(pieces, axis=1) if len(pieces) > 1 else pieces[0]

    get_x.wait()
    get_b.wait()
    get_c.wait()

    @pl.when(e > 0)
    def _():
        for copy in halo:
            copy.wait_recv()

    x_w = xtaps[...].astype(F32)
    bc_w = jnp.concatenate([btaps[:, lane_b], ctaps[:, lane_b]], axis=1).astype(F32)
    lane2 = lax.broadcasted_iota(jnp.int32, (1, 2 * LANES), 1) % LANES
    in_group = (lane2 >= within) & (lane2 < within + STATE)
    taps = x_w.shape[0]

    def conv(ref, w, k):
        v = ref[pl.ds(pl.multiple_of(k * BLOCK, BLOCK), BLOCK + HALO), :].astype(F32)
        total = v[HALO:] * w[taps - 1 :]
        for j in range(taps - 1):
            total = total + pltpu.roll(v, taps - 1 - j, 0)[HALO:] * w[j : j + 1]
        return silu(total)

    st_s[...] = jnp.zeros_like(st_s)
    dec_s[...] = jnp.ones_like(dec_s)

    def first_pass(k, carry):
        rows = pl.ds(pl.multiple_of(k * BLOCK, BLOCK), BLOCK)
        xs = conv(xpad, x_w, k).astype(BF16)
        bc = jnp.where(in_group, conv(bcpad, bc_w, k), 0.0).astype(BF16)
        xs_s[rows, :] = xs
        bc_s[rows, :] = bc
        cols = jnp.transpose(rows_s[k])
        xw = (xs.astype(F32) * spread(cols, 16)).astype(BF16)
        block_state = dot(bc[:, :LANES], xw, (((0,), (0,)), ((), ())))
        gone = spread(cols[BLOCK - 8 :, :], 24)[7:8, :]
        prev_s[k] = st_s[...]
        dpre_s[k] = dec_s[...]
        st_s[...] = st_s[...] * gone + block_state
        dec_s[...] = dec_s[...] * gone
        return carry

    lax.fori_loop(0, nblk, first_pass, 0)

    def weight_view(block, way, k, d):
        slab = wk.at[block, across_z(k)]
        if d == half_ring:
            return slab.at[pl.ds(way * (rows_w // 2), rows_w // 2), :]
        return slab

    def send_weight(way, d, k):
        view = weight_view(at_ring(-(d - 1) if way == 0 else d - 1), way, k, d)
        send(view, view, wr_s.at[way, d - 1, k - 1], wr_r.at[way, d - 1, k - 1], toward[way])

    def first_weight(k):
        arrived(wk.at[e, across_z(k)], wz_r.at[k - 1])
        for way in range(2):
            send_weight(way, 1, k)

    def weight_arrived(way, d, k):
        view = weight_view(at_ring(-d if way == 0 else d), way, k, d)
        arrived(view, wr_r.at[way, d - 1, k - 1])

    def pass_weight(d, k):
        for way in range(2):
            weight_arrived(way, d, k)
            send_weight(way, d + 1, k)

    group_rows = pl.ds(pl.multiple_of(within, STATE), STATE)
    smsg[0:STATE, :] = st_s[group_rows, :].astype(BF16)
    smsg[STATE : STATE + 16, :] = jnp.concatenate([dec_s[...]] * 2, axis=0).astype(BF16)
    state_copies = [
        remote(smsg, srecv.at[k], state_s.at[k], state_r.at[k], ((e + 1 + k) % n_ep, t))
        for k in range(n_ep - 1)
    ]
    for k, copy in enumerate(state_copies):
        pl.when(e + 1 + k < n_ep)(copy.start)
    for way in range(2):
        send_tokens(way, 1, 2)
    get_eg.wait()
    get_eu.wait()
    get_ed.wait()
    experts(e, 0)
    share_tokens(1, [0])
    share_tokens(1, [1])

    def order_of(way, d):
        if d == half_ring:
            return 2 * d - 1
        if d == 0:
            return 0
        return 2 * d - 1 + way

    def partner_sum(block, order):
        arrived(precv.at[block], pd_r.at[order])

    keep = feats * n_z
    keep_half = keep // 2

    def ring_sum(d, way):
        block = at_ring(d if way == 0 else -d)
        if d == half_ring:
            cols = pl.ds(way * keep_half, keep_half)
            value = pmine[block, :, cols].astype(F32) + precv[block, :, cols].astype(F32)
            pmine[block, :, cols] = value.astype(BF16)
            view = pmine.at[block, :, cols]
            send(
                view, rsrecv.at[way, d - 1, :, cols], rs_s.at[way, d - 1], rs_r.at[way, d - 1], toward[way]
            )
            return
        last = d == half_ring - 1
        cols = pl.ds(way * keep_half, keep_half) if last else pl.ds(0, keep)
        arrived(rsrecv.at[way, d, :, cols], rs_r.at[way, d])
        if last:
            rest = pl.ds((1 - way) * keep_half, keep_half)
            pmine[block, :, rest] = (
                pmine[block, :, rest].astype(F32) + precv[block, :, rest].astype(F32)
            ).astype(BF16)
        pmine[block, :, cols] = (
            pmine[block, :, cols].astype(F32)
            + precv[block, :, cols].astype(F32)
            + rsrecv[way, d, :, cols].astype(F32)
        ).astype(BF16)
        send(
            pmine.at[block], rsrecv.at[way, d - 1], rs_s.at[way, d - 1], rs_r.at[way, d - 1], toward[way]
        )

    ent[...] = jnp.zeros_like(ent)
    for k in reversed(range(n_ep - 1)):

        @pl.when(e > k)
        def _(k=k):
            arrived(srecv.at[k], state_r.at[k])
            before = ent[group_rows, :]
            gone = srecv[k, STATE : STATE + 16, :].astype(F32)[0:1, :]
            ent[group_rows, :] = before * gone + srecv[k, 0:STATE, :].astype(F32)

    get_gate.wait()
    head_lane = lax.broadcasted_iota(jnp.int32, (1, width), 1) // STATE
    d_row = jnp.zeros((1, width), F32)
    for h in range(heads):
        d_row = jnp.where(head_lane == h, dscale[h], d_row)
    g_row = gnorm[...].astype(F32).reshape(1, width)
    row_id = lax.broadcasted_iota(jnp.int32, (BLOCK, BLOCK), 0)
    col_id = lax.broadcasted_iota(jnp.int32, (BLOCK, BLOCK), 1)
    same_head = (
        lax.broadcasted_iota(jnp.int32, (width, width), 0) // STATE
        == lax.broadcasted_iota(jnp.int32, (width, width), 1) // STATE
    )
    mean_of = jnp.where(same_head, 1.0 / STATE, 0.0).astype(BF16)

    def second_pass(k):
        rows = pl.ds(pl.multiple_of(k * BLOCK, BLOCK), BLOCK)
        xs_f = xs_s[rows, :].astype(F32)
        bs = bc_s[rows, pl.ds(0, LANES)]
        cs = bc_s[rows, pl.ds(LANES, LANES)]
        row_q = rows_s[k]
        cols = jnp.transpose(row_q)
        scores = dot(cs, bs, (((1,), (1,)), ((), ())))
        x_dt = (xs_f * spread(cols, 8)).astype(BF16)
        inner = []
        for j in range(width // LANES):
            both = []
            for h in (2 * j, 2 * j + 1):
                diff = cols[:, h : h + 1] - row_q[h : h + 1, :]
                link = jnp.exp(jnp.where(row_id >= col_id, diff, -1e30))
                both.append(dot((scores * link).astype(BF16), x_dt[:, j * LANES : (j + 1) * LANES]))
            inner.append(jnp.where(lane < STATE, both[0], both[1]))
        inner = jnp.concatenate(inner, axis=1) if len(inner) > 1 else inner[0]
        prev = prev_s[k] + ent[...] * dpre_s[k, 0:1, :]
        carried = dot(cs, prev.astype(BF16)) * spread(cols, 24)
        gated = (inner + carried + d_row * xs_f) * silu(gate[rows, :].astype(F32))
        square = gated * gated
        high = square.astype(BF16)
        low = (square - high.astype(F32)).astype(BF16)
        mean = dot(high, mean_of) + dot(low, mean_of)
        mixed[rows, :] = (gated * lax.rsqrt(mean + EPS) * g_row).astype(BF16)

    chip_rows = rows_dev * CORES
    per_chip = chip_rows // BLOCK

    def mix_for(k):
        target = across_z(k)

        def body(i, carry):
            second_pass(target * per_chip + i)
            return carry

        lax.fori_loop(0, per_chip, body, 0)
        view = mixed.at[pl.ds(pl.multiple_of(target * chip_rows, chip_rows), chip_rows), :]
        if k:
            send(view, mrecv.at[z], a2a_s.at[k - 1], a2a_r.at[k - 1], z_device(k))
        else:
            own = pl.ds(pl.multiple_of(z * chip_rows, chip_rows), chip_rows)
            mrecv[z] = mixed[own, :]

    def ring_step(d):
        for way in range(2):
            partner_sum(at_ring(d if way == 0 else -d), order_of(1 - way, d))
            ring_sum(d, way)

    mixes = [k for k in range(2, n_z)] + [1, 0]
    mix_for(mixes.pop(0))
    waiting = list(z_order)
    share_tokens(1, [2])
    first_weight(waiting.pop(0))
    for k in range(1, n_ep):
        arrived(wts.at[(e - k + n_ep) % n_ep], wts_r.at[k - 1])
    for d in range(1, half_ring + 1):
        if 1 < d < half_ring:
            share_tokens(d, pieces_of(d))
        for way in range(2):
            shared_tokens(way, d)
        if d < half_ring:
            for way in range(2):
                experts(at_ring(-d if way == 0 else d), order_of(way, d))
                if way == 0 and d + 1 == half_ring:
                    share_tokens(half_ring, pieces_of(half_ring))
        else:
            experts(at_ring(d), order_of(0, d))
    partner_sum(at_ring(half_ring), order_of(0, half_ring))
    for way in range(2):
        ring_sum(half_ring, way)
    first_weight(waiting.pop(0))
    mix_for(mixes.pop(0))
    for d in range(half_ring - 1, 0, -1):
        if mixes:
            mix_for(mixes.pop(0))
        ring_step(d)
    while waiting:
        first_weight(waiting.pop(0))
    for k in mixes:
        mix_for(k)

    for d in range(1, half_ring):
        for k in z_order[:-1]:
            pass_weight(d, k)

    partner_sum(e, 0)
    for way in range(2):
        arrived(rsrecv.at[way, 0], rs_r.at[way, 0])

    def own_sum(target):
        at = pl.ds(pl.multiple_of(target * feats, feats), feats)
        return (
            pmine[e, :, at].astype(F32)
            + precv[e, :, at].astype(F32)
            + rsrecv[0, 0, :, at].astype(F32)
            + rsrecv[1, 0, :, at].astype(F32)
        )

    for k in range(1, n_z):
        target = across_z(k)
        zsend[k - 1] = own_sum(target).astype(BF16)
        send(zsend.at[k - 1], zrecv.at[k - 1], zs_s.at[k - 1], zs_r.at[k - 1], z_device(k))

    for d in range(1, half_ring):
        pass_weight(d, z_order[-1])

    for k in range(1, n_z):
        arrived(mrecv.at[across_z(k)], a2a_r.at[k - 1])
    for copy in get_w:
        copy.wait()

    def rows_of(core):
        return pl.ds(pl.multiple_of(core * rows_dev, rows_dev), rows_dev)

    def product(core, block):
        total = dot(mrecv[0, rows_of(core), :], wk[block, 0])
        for k in range(1, n_z):
            total = total + dot(mrecv[k, rows_of(core), :], wk[block, k])
        return total

    def give(order):
        send(pjsend.at[order], pjrecv.at[order], pj_s.at[order], pj_r.at[order], partner)

    def project(block, order):
        pjsend[order] = product(1 - c, block).astype(BF16)
        give(order)
        pjown[order] = product(c, block)

    def project_late(block, order):
        both = (c, 1 - c)
        for core, total in zip(both, (pjown.at[order], pjlast)):
            total[...] = dot(mrecv[z, rows_of(core), :], wk[block, z])
        for k in z_order:
            for way in range(2):
                weight_arrived(way, half_ring, k)
            place = across_z(k)
            if k == z_order[-1]:
                total = pjlast[...] + dot(mrecv[place, rows_of(1 - c), :], wk[block, place])
                pjsend[order] = total.astype(BF16)
                give(order)
                pjown[order] += dot(mrecv[place, rows_of(c), :], wk[block, place])
            else:
                for core, total in zip(both, (pjown.at[order], pjlast)):
                    total[...] += dot(mrecv[place, rows_of(core), :], wk[block, place])

    puts = []

    def put(src, dst, index):
        copy = pltpu.make_async_copy(src, dst, ld.at[index])
        copy.start()
        puts.append(copy)

    def finish(block, order):
        arrived(pjrecv.at[order], pj_r.at[order])
        result[order] = (pjown[order] + pjrecv[order].astype(F32)).astype(BF16)
        cols = pl.ds(pl.multiple_of(block * part, part), part)
        put(result.at[order], out.at[:, cols], order)

    project(e, 0)
    done = [(e, 0)]
    for d in range(1, half_ring):
        for way in range(2):
            block = at_ring(-d if way == 0 else d)
            project(block, order_of(way, d))
            done.append((block, order_of(way, d)))

    total = own_sum(z)
    for k in range(1, n_z):
        arrived(zrecv.at[k - 1], zs_r.at[k - 1])
        total = total + zrecv[k - 1].astype(F32)
    eresult[...] = total.astype(BF16)
    put(eresult, eout, n_ep)

    for block, order in done:
        finish(block, order)
    project_late(at_ring(half_ring), order_of(0, half_ring))
    finish(at_ring(half_ring), order_of(0, half_ring))

    for copy in pending:
        copy.wait_send()
    for copy in puts:
        copy.wait()

    @pl.when(e < n_ep - 1)
    def _():
        for copy in halo:
            copy.wait_send()

    for k, copy in enumerate(state_copies):
        pl.when(e + 1 + k < n_ep)(copy.wait_send)


def hand_over_kernel(chunks, a_in, b_in, a_out, b_out, a, b, sems):
    rows = a.shape[0] // chunks
    moves = [(a_in.at[pl.ds(i * rows, rows)], a.at[pl.ds(i * rows, rows)], a_out.at[pl.ds(i * rows, rows)]) for i in range(chunks)]
    moves.append((b_in, b, b_out))
    reads = [pltpu.make_async_copy(m[0], m[1], sems.at[0, i]) for i, m in enumerate(moves)]
    writes = [pltpu.make_async_copy(m[1], m[2], sems.at[1, i]) for i, m in enumerate(moves)]
    for copy in reads:
        copy.start()
    for read, write in zip(reads, writes):
        read.wait()
        write.start()
    for copy in writes:
        copy.wait()


def hand_over(a, b):
    chunks = 4
    anywhere = pl.BlockSpec(memory_space=pl.ANY)
    return pl.pallas_call(
        functools.partial(hand_over_kernel, chunks),
        out_shape=(jax.ShapeDtypeStruct(a.shape, a.dtype), jax.ShapeDtypeStruct(b.shape, b.dtype)),
        in_specs=[anywhere] * 2,
        out_specs=(anywhere, anywhere),
        scratch_shapes=[
            pltpu.VMEM(a.shape, a.dtype),
            pltpu.VMEM(b.shape, b.dtype),
            pltpu.SemaphoreType.DMA((2, chunks + 1)),
        ],
        name="hand_over",
    )(a, b)


def fused(n_ep, n_tp, args):
    (
        x,
        gate_logits,
        b_map,
        c_map,
        xtaps,
        btaps,
        ctaps,
        step,
        lograte,
        extra,
        dscale,
        gnorm,
        wout,
        tokens,
        pnorm,
        group_cols,
        expert_cols,
        routes,
        eg,
        eu,
        ed,
    ) = args
    n_z = n_tp // CORES
    half_ring = n_ep // 2
    length, width = x.shape
    heads = dscale.shape[0]
    nblk = length // BLOCK
    n_tok, depth = tokens.shape
    feats = depth // n_tp
    ff = eg.shape[2]
    rows_w, cols_w = wout.shape
    part = cols_w // n_ep
    rows_dev = length // n_tp
    chip_rows = rows_dev * CORES
    w_rows = -(-expert_cols.shape[1] // 8) * 8
    slots = max(2, min(n_ep, 16 // n_ep))
    keep = n_z * feats
    anywhere = pl.BlockSpec(memory_space=pl.ANY)
    vmem = pl.BlockSpec(memory_space=pltpu.VMEM)
    smem = pl.BlockSpec(memory_space=pltpu.SMEM)
    dma = pltpu.SemaphoreType.DMA
    scratch = [
        pltpu.VMEM((length + HALO, width), BF16),
        pltpu.VMEM((length + HALO, 2 * LANES), BF16),
        pltpu.VMEM((length, width), BF16),
        pltpu.VMEM((depth, ff), BF16),
        pltpu.VMEM((depth, ff), BF16),
        pltpu.VMEM((ff, depth), BF16),
        pltpu.VMEM((n_ep, n_z, rows_w, part), BF16),
        pltpu.VMEM((n_ep, n_tok, depth), BF16),
        pltpu.VMEM((n_ep, w_rows, n_tok), F32),
        pltpu.VMEM((n_tok, ff), BF16),
        pltpu.VMEM((slots, n_tok, keep), BF16),
        pltpu.VMEM((n_ep, n_tok, keep), BF16),
        pltpu.VMEM((n_ep, n_tok, keep), BF16),
        pltpu.VMEM((2, half_ring, n_tok, keep), BF16),
        pltpu.VMEM((n_z - 1, n_tok, feats), BF16),
        pltpu.VMEM((n_z - 1, n_tok, feats), BF16),
        pltpu.VMEM((length, width), BF16),
        pltpu.VMEM((length, 2 * LANES), BF16),
        pltpu.VMEM((nblk, BLOCK, BLOCK), F32),
        pltpu.VMEM((nblk, LANES, width), F32),
        pltpu.VMEM((nblk, 8, width), F32),
        pltpu.VMEM((LANES, width), F32),
        pltpu.VMEM((8, width), F32),
        pltpu.VMEM((STATE + 16, width), BF16),
        pltpu.VMEM((n_ep - 1, STATE + 16, width), BF16),
        pltpu.VMEM((LANES, width), F32),
        pltpu.VMEM((length, width), BF16),
        pltpu.VMEM((n_z, chip_rows, width), BF16),
        pltpu.VMEM((n_ep, rows_dev, part), BF16),
        pltpu.VMEM((n_ep, rows_dev, part), F32),
        pltpu.VMEM((rows_dev, part), F32),
        pltpu.VMEM((n_ep, rows_dev, part), BF16),
        pltpu.VMEM((n_ep, rows_dev, part), BF16),
        pltpu.VMEM((n_tok, feats), BF16),
        dma((8 + n_ep,)),
        dma((3,)),
        dma((3,)),
    ]
    for shape in (
        (2, half_ring, 3),
        (2, half_ring, 3),
        (n_ep - 1,),
        (n_z - 1,),
        (2, half_ring, n_z - 1),
        (n_ep - 1,),
        (n_ep,),
        (2, half_ring),
        (n_z - 1,),
        (n_z - 1,),
        (n_ep,),
    ):
        scratch += [dma(shape), dma(shape)]
    mixer_out, experts_out = pl.pallas_call(
        functools.partial(kernel, n_ep, n_tp),
        out_shape=(
            jax.ShapeDtypeStruct((rows_dev, cols_w), BF16),
            jax.ShapeDtypeStruct((n_tok, feats), BF16),
        ),
        in_specs=[anywhere] * 9 + [vmem] * 5 + [smem] * 2 + [vmem] * 5,
        out_specs=(anywhere, anywhere),
        scratch_shapes=scratch,
        name="fused",
        compiler_params=pltpu.CompilerParams(
            collective_id=0, has_side_effects=True, vmem_limit_bytes=67_000_000
        ),
    )(
        x,
        gate_logits,
        b_map,
        c_map,
        wout,
        tokens,
        eg[0],
        eu[0],
        ed[0],
        xtaps,
        btaps,
        ctaps,
        step,
        extra,
        lograte,
        dscale,
        gnorm,
        pnorm,
        group_cols.T,
        expert_cols.T,
        routes.T,
    )
    return hand_over(mixer_out, experts_out)


def solution(mesh):
    n_ep, n_tp = mesh.shape["ep"], mesh.shape["tp"]
    in_specs = (
        P("ep", "tp"),
        P("ep", "tp"),
        P("ep", None),
        P("ep", None),
        P(None, "tp"),
        P(),
        P(),
        P("tp", "ep"),
        P("tp"),
        P("tp", "ep"),
        P("tp"),
        P("tp"),
        P("tp", None),
        P("ep", None),
        P(),
        P(),
        P(),
        P("ep", None),
        P("ep", None, "tp"),
        P("ep", None, "tp"),
        P("ep", "tp", None),
    )
    out_specs = (P(("ep", "tp"), None), P("ep", "tp"))
    return jax.shard_map(
        lambda *args: fused(n_ep, n_tp, args),
        mesh=mesh,
        in_specs=in_specs,
        out_specs=out_specs,
        check_vma=False,
    )
```

```python
import functools
import math

import jax
import jax.numpy as jnp
from jax import lax
from jax.experimental import pallas as pl
from jax.experimental.pallas import tpu as pltpu
from jax.sharding import PartitionSpec as P

STATE = 64
GROUPS = 4
HEADS = 32
BLOCK = 128
CORES = 2
LANES = 128
HALO = 16
EPS = 1e-6
MESH = pl.DeviceIdType.MESH
F32 = jnp.float32
BF16 = jnp.bfloat16


def snake(i, n):
    w = math.isqrt(n)
    y, x = i // w, i % w
    odd = y % 2
    return y * w + x * (1 - 2 * odd) + odd * (w - 1)


def silu(v):
    return v / (1.0 + jnp.exp(-v))


def dot(a, b, dims=(((1,), (0,)), ((), ()))):
    return lax.dot_general(a, b, dims, preferred_element_type=F32)


def kernel(
    n_ep,
    n_tp,
    x_hbm,
    gate_hbm,
    b_hbm,
    c_hbm,
    wout_hbm,
    tok_hbm,
    eg_hbm,
    eu_hbm,
    ed_hbm,
    xtaps_hbm,
    btaps_hbm,
    ctaps_hbm,
    step_hbm,
    extra_hbm,
    lograte_hbm,
    dscale_hbm,
    gnorm_hbm,
    pnorm_hbm,
    grouter_hbm,
    erouter_hbm,
    routes_hbm,
    out,
    eout,
    xtaps,
    btaps,
    ctaps,
    step,
    extra,
    lograte,
    dscale,
    gnorm,
    pnorm,
    grouter,
    erouter,
    routes,
    xpad,
    bcpad,
    gate,
    eg,
    eu,
    ed,
    wk,
    rows_tok,
    wts,
    hid,
    psend,
    pmine,
    precv,
    rsrecv,
    zsend,
    zrecv,
    xs_s,
    bc_s,
    rows_s,
    prev_s,
    dpre_s,
    st_s,
    dec_s,
    smsg,
    srecv,
    ent,
    mixed,
    mrecv,
    pjsend,
    pjown,
    pjlast,
    pjrecv,
    result,
    eresult,
    eown,
    ld,
    halo_s,
    halo_r,
    tok_s,
    tok_r,
    tokp_s,
    tokp_r,
    wts_s,
    wts_r,
    wz_s,
    wz_r,
    wr_s,
    wr_r,
    wx_s,
    wx_r,
    state_s,
    state_r,
    pd_s,
    pd_r,
    rs_s,
    rs_r,
    rsl_s,
    rsl_r,
    zs_s,
    zs_r,
    a2a_s,
    a2a_r,
    pj_s,
    pj_r,
):
    n_z = n_tp // CORES
    half_ring = n_ep // 2
    e = lax.axis_index("ep")
    t = lax.axis_index("tp")
    c = t % CORES
    z = t // CORES
    ring = snake(e, n_ep)
    partner = (e, t + 1 - 2 * c)

    def across_z(k):
        place, bit = 0, 1
        while bit < n_z:
            own = z // bit % 2
            place = place + bit * ((1 - own) if k & bit else own)
            bit *= 2
        return place

    def z_device(k):
        return (e, CORES * across_z(k) + c)

    def at_ring(offset):
        return snake((ring + offset + n_ep) % n_ep, n_ep)

    next_ep, prev_ep = at_ring(1), at_ring(-1)
    toward = ((next_ep, t), (prev_ep, t))
    length, width = x_hbm.shape
    heads = width // STATE
    nblk = length // BLOCK
    group = t * heads // (HEADS // GROUPS)
    pair = group * STATE // LANES
    within = group * STATE % LANES
    n_tok, depth = tok_hbm.shape
    half = n_tok // CORES
    quarter = half // 2
    feats = depth // n_tp
    ff = eg_hbm.shape[1]
    rows_w = wout_hbm.shape[0]
    part = wout_hbm.shape[1] // n_ep
    rows_dev = out.shape[0]
    pending = []

    def remote(src, dst, send, recv, device):
        return pltpu.make_async_remote_copy(
            src_ref=src, dst_ref=dst, send_sem=send, recv_sem=recv, device_id=device, device_id_type=MESH
        )

    def send(src, dst, send_sem, recv_sem, device):
        copy = remote(src, dst, send_sem, recv_sem, device)
        copy.start()
        pending.append(copy)
        return copy

    def arrived(view, sem):
        remote(view, view, sem, sem, partner).wait_recv()

    def local(src, dst, index):
        copy = pltpu.make_async_copy(src, dst, ld.at[index])
        copy.start()
        return copy

    get_tok = [
        local(tok_hbm.at[rows], rows_tok.at[e, rows], i)
        for i, rows in enumerate(
            pl.ds(pl.multiple_of(core * (tok_hbm.shape[0] // CORES), 32), tok_hbm.shape[0] // CORES)
            for core in (c, 1 - c)
        )
    ]
    get_pnorm = local(pnorm_hbm, pnorm, 19 + n_ep)
    get_eg = local(eg_hbm, eg, 20 + n_ep)
    get_eu = local(eu_hbm, eu, 2)
    get_ed = local(ed_hbm, ed, 3)
    lane_b = pl.ds(pl.multiple_of(pair * LANES, LANES), LANES)
    get_x = local(x_hbm, xpad.at[pl.ds(HALO, length)], 4)
    get_b = local(b_hbm.at[:, lane_b], bcpad.at[pl.ds(HALO, length), pl.ds(0, LANES)], 5)
    get_c = local(c_hbm.at[:, lane_b], bcpad.at[pl.ds(HALO, length), pl.ds(LANES, LANES)], 6)
    get_gate = local(gate_hbm, gate, 7)
    get_w = [
        local(wout_hbm.at[:, pl.ds(q * part, part)], wk.at[q, z], 8 + q) for q in range(n_ep)
    ]

    get_small = [
        local(src, dst, 8 + n_ep + i)
        for i, (src, dst) in enumerate(
            (
                (grouter_hbm, grouter),
                (erouter_hbm, erouter),
                (routes_hbm, routes),
                (step_hbm, step),
                (extra_hbm, extra),
                (lograte_hbm, lograte),
                (xtaps_hbm, xtaps),
                (btaps_hbm, btaps),
                (ctaps_hbm, ctaps),
                (dscale_hbm, dscale),
                (gnorm_hbm, gnorm),
            )
        )
    ]

    barrier = pltpu.get_barrier_semaphore()
    peers = 0
    for k in range(1, n_ep):
        pl.semaphore_signal(barrier, inc=1, device_id=((e + k) % n_ep, t), device_id_type=MESH)
        peers += 1
    for k in range(1, n_z):
        pl.semaphore_signal(barrier, inc=1, device_id=z_device(k), device_id_type=MESH)
        peers += 1
    pl.semaphore_signal(barrier, inc=1, device_id=partner, device_id_type=MESH)
    peers += 1

    get_pnorm.wait()
    get_tok[0].wait()
    scale = pnorm[...].astype(F32).reshape(1, depth)

    def norm_rows(i, carry):
        rows = pl.ds(pl.multiple_of(i * 32, 32), 32)
        v = rows_tok[e, rows, :].astype(F32)
        v = v * lax.rsqrt(jnp.mean(v * v, axis=-1, keepdims=True) + EPS) * scale
        rows_tok[e, rows, :] = v.astype(BF16)
        return carry

    steps = half // 32
    lax.fori_loop(c * steps, c * steps + steps, norm_rows, 0)

    pl.semaphore_wait(barrier, peers)

    def tok_view(core, way, d, piece):
        block = at_ring(-d if way == 0 else d)
        if piece == 0:
            first, count = core * half + way * quarter, quarter
        else:
            count = quarter // 2
            first = core * half + (1 - way) * quarter + (piece - 1) * count
        return rows_tok.at[block, pl.ds(pl.multiple_of(first, count), count), :]

    def pieces_of(d):
        return range(1 if d == half_ring else 3)

    def send_tokens(way, d, piece):
        view = tok_view(c, way, d - 1, piece)
        send(view, view, tok_s.at[way, d - 1, piece], tok_r.at[way, d - 1, piece], toward[way])

    def share_tokens(d, pieces):
        for piece in pieces:
            for way in range(2):
                view = tok_view(c, way, d, piece)
                arrived(view, tok_r.at[way, d - 1, piece])
                if d < half_ring and piece in pieces_of(d + 1):
                    send_tokens(way, d + 1, piece)
                send(view, view, tokp_s.at[way, d - 1, piece], tokp_r.at[way, d - 1, piece], partner)

    def shared_tokens(way, d):
        for piece in pieces_of(d):
            arrived(tok_view(1 - c, way, d, piece), tokp_r.at[way, d - 1, piece])

    tail_rows = pl.ds(length - HALO, HALO)
    head_rows = pl.ds(0, HALO)
    halo = [
        remote(src, dst, halo_s.at[i], halo_r.at[i], ((e + 1) % n_ep, t))
        for i, (src, dst) in enumerate(
            (
                (x_hbm.at[tail_rows], xpad.at[head_rows]),
                (b_hbm.at[tail_rows, lane_b], bcpad.at[head_rows, pl.ds(0, LANES)]),
                (c_hbm.at[tail_rows, lane_b], bcpad.at[head_rows, pl.ds(LANES, LANES)]),
            )
        )
    ]

    @pl.when(e < n_ep - 1)
    def _():
        for copy in halo:
            copy.start()

    @pl.when(e == 0)
    def _():
        xpad[head_rows, :] = jnp.zeros((HALO, width), BF16)
        bcpad[head_rows, :] = jnp.zeros((HALO, 2 * LANES), BF16)

    for piece in pieces_of(1):
        for way in range(2):
            send_tokens(way, 1, piece)

    mine = pl.ds(pl.multiple_of(e * part, part), part)
    z_order = sorted(range(1, n_z), key=lambda k: (k != 1, -k))

    def weight_along_z(k):
        send(wout_hbm.at[:, mine], wk.at[e, z], wz_s.at[k - 1], wz_r.at[k - 1], z_device(k))

    for k in z_order[:-1]:
        weight_along_z(k)

    get_tok[1].wait()
    for copy in get_small:
        copy.wait()
    lax.fori_loop((1 - c) * steps, (1 - c) * steps + steps, norm_rows, 0)

    for way in range(2):
        rest = pl.ds((1 - way) * (n_z * feats // 2), n_z * feats // 2)
        rsrecv[way, half_ring - 1, :, rest] = jnp.zeros((n_tok, n_z * feats // 2), BF16)

    n_experts, n_grp = erouter.shape[0], grouter.shape[0]
    over_rows = (((1,), (1,)), ((), ()))
    logits = dot(erouter[...], rows_tok[e], over_rows)
    expert_logit = [logits[i : i + 1, :] for i in range(n_experts)]
    logits = dot(grouter[...], rows_tok[e], over_rows)
    per_group = n_experts // n_grp
    group_logit = [logits[i : i + 1, :] for i in range(n_grp)]

    def log_softmax(rows):
        top = functools.reduce(jnp.maximum, rows)
        norm = jnp.log(functools.reduce(jnp.add, [jnp.exp(v - top) for v in rows]))
        return [v - top - norm for v in rows]

    group_lp = log_softmax(group_logit)
    total_lp = []
    for i in range(n_grp):
        inner = log_softmax(expert_logit[i * per_group : (i + 1) * per_group])
        total_lp += [group_lp[i] + v for v in inner]
    picks = [routes[k : k + 1, :] for k in range(2)]
    chosen = []
    for k in range(2):
        value = jnp.zeros_like(total_lp[0])
        for i in range(n_experts):
            value = jnp.where(picks[k] == i, total_lp[i], value)
        chosen.append(value)
    top = jnp.maximum(chosen[0], chosen[1])
    share = [jnp.exp(v - top) for v in chosen]
    inv = 1.0 / (share[0] + share[1])
    share = [v * inv for v in share]
    wts[e] = jnp.zeros(wts.shape[1:], F32)
    for i in range(n_experts):
        wts[e, i : i + 1, :] = jnp.where(picks[0] == i, share[0], 0.0) + jnp.where(
            picks[1] == i, share[1], 0.0
        )
    for k in range(1, n_ep):
        send(wts.at[e], wts.at[e], wts_s.at[k - 1], wts_r.at[k - 1], ((e + k) % n_ep, t))

    slots = psend.shape[0]
    to_partner = {}

    def experts(block, order):
        wrow = wts[block, pl.ds(e, 1), :]
        wcol = jnp.transpose(jnp.broadcast_to(wrow, (LANES, n_tok)))
        wide = 256
        wcol = jnp.concatenate([wcol] * (wide // LANES), axis=1)

        def up(j, carry):
            cols = pl.ds(pl.multiple_of(j * wide, wide), wide)
            g = dot(rows_tok[block], eg[:, cols])
            u = dot(rows_tok[block], eu[:, cols])
            hid[:, cols] = (silu(g) * u * wcol).astype(BF16)
            return carry

        lax.fori_loop(0, ff // wide, up, 0)
        slot = order % slots
        if order >= slots:
            earlier = to_partner[order - slots]
            earlier.wait_send()
            pending[:] = [copy for copy in pending if copy is not earlier]

        def down(into, core):
            for k in range(n_z):
                at = pl.ds(k * feats, feats)
                cols = pl.ds(pl.multiple_of((CORES * k + core) * feats, feats), feats)
                into[:, at] = dot(hid[...], ed[:, cols]).astype(BF16)

        down(psend.at[slot], 1 - c)
        to_partner[order] = send(
            psend.at[slot], precv.at[block], pd_s.at[order], pd_r.at[order], partner
        )
        down(pmine.at[block], c)

    lane = lax.broadcasted_iota(jnp.int32, (1, LANES), 1)
    head_row = lax.broadcasted_iota(jnp.int32, (heads, 1), 0)
    rate = jnp.zeros((heads, 1), F32)
    for h in range(heads):
        rate = jnp.where(head_row == h, lograte[h], rate)
    rate = jnp.exp(rate)
    for k in range(nblk):
        at = pl.ds(k * BLOCK, BLOCK)
        v = step[:, at]
        dt = jnp.maximum(v, 0.0) + jnp.log(1.0 + jnp.exp(-jnp.abs(v)))
        cum = extra[:, at] - dt * rate
        hop = 1
        while hop < BLOCK:
            cum = cum + jnp.where(lane >= hop, pltpu.roll(cum, hop, 1), 0.0)
            hop *= 2
        grown = jnp.exp(cum)
        left = jnp.exp(cum[:, BLOCK - 1 :] - cum) * dt
        rows_s[k, 0:heads, :] = cum
        rows_s[k, 8 : 8 + heads, :] = dt
        rows_s[k, 16 : 16 + heads, :] = left
        rows_s[k, 24 : 24 + heads, :] = grown

    def spread(cols, first):
        pieces = []
        for j in range(width // LANES):
            low = cols[:, first + 2 * j : first + 2 * j + 1]
            high = cols[:, first + 2 * j + 1 : first + 2 * j + 2]
            pieces.append(jnp.where(lane < STATE, low, high))
        return jnp.concatenate(pieces, axis=1) if len(pieces) > 1 else pieces[0]

    get_x.wait()
    get_b.wait()
    get_c.wait()

    @pl.when(e > 0)
    def _():
        for copy in halo:
            copy.wait_recv()

    x_w = xtaps[...].astype(F32)
    bc_w = jnp.concatenate([btaps[:, lane_b], ctaps[:, lane_b]], axis=1).astype(F32)
    lane2 = lax.broadcasted_iota(jnp.int32, (1, 2 * LANES), 1) % LANES
    in_group = (lane2 >= within) & (lane2 < within + STATE)
    taps = x_w.shape[0]

    def conv(ref, w, k):
        v = ref[pl.ds(pl.multiple_of(k * BLOCK, BLOCK), BLOCK + HALO), :].astype(F32)
        total = v[HALO:] * w[taps - 1 :]
        for j in range(taps - 1):
            total = total + pltpu.roll(v, taps - 1 - j, 0)[HALO:] * w[j : j + 1]
        return silu(total)

    st_s[...] = jnp.zeros_like(st_s)
    dec_s[...] = jnp.ones_like(dec_s)

    def first_pass(k, carry):
        rows = pl.ds(pl.multiple_of(k * BLOCK, BLOCK), BLOCK)
        xs = conv(xpad, x_w, k).astype(BF16)
        bc = jnp.where(in_group, conv(bcpad, bc_w, k), 0.0).astype(BF16)
        xs_s[rows, :] = xs
        bc_s[rows, :] = bc
        cols = jnp.transpose(rows_s[k])
        xw = (xs.astype(F32) * spread(cols, 16)).astype(BF16)
        block_state = dot(bc[:, :LANES], xw, (((0,), (0,)), ((), ())))
        gone = spread(cols[BLOCK - 8 :, :], 24)[7:8, :]
        prev_s[k] = st_s[...]
        dpre_s[k] = dec_s[...]
        st_s[...] = st_s[...] * gone + block_state
        dec_s[...] = dec_s[...] * gone
        return carry

    lax.fori_loop(0, nblk, first_pass, 0)

    half_w = rows_w // 2

    def weight_view(block, way, k, d):
        slab = wk.at[block, across_z(k)]
        if d == half_ring:
            return slab.at[pl.ds(way * half_w, half_w), :]
        return slab.at[pl.ds(0, half_w), :] if k == 1 else slab

    def on_ring(d, k):
        return k != 1 or d < half_ring

    def send_weight(way, d, k):
        if on_ring(d, k):
            view = weight_view(at_ring(-(d - 1) if way == 0 else d - 1), way, k, d)
            send(view, view, wr_s.at[way, d - 1, k - 1], wr_r.at[way, d - 1, k - 1], toward[way])

    def first_weight(k):
        arrived(wk.at[e, across_z(k)], wz_r.at[k - 1])
        for way in range(2):
            send_weight(way, 1, k)

    def weight_arrived(way, d, k):
        if on_ring(d, k):
            view = weight_view(at_ring(-d if way == 0 else d), way, k, d)
            arrived(view, wr_r.at[way, d - 1, k - 1])

    def pass_weight(d, k):
        for way in range(2):
            weight_arrived(way, d, k)
            send_weight(way, d + 1, k)

    def direct_rows(d):
        return pl.ds(0, rows_w) if d == half_ring else pl.ds(half_w, rows_w - half_w)

    def direct_weight(block, order, d):
        cols = pl.ds(pl.multiple_of(block * part, part), part)
        send(
            wout_hbm.at[direct_rows(d), cols],
            wk.at[block, z, direct_rows(d), :],
            wx_s.at[order - 1],
            wx_r.at[order - 1],
            z_device(1),
        )

    def direct_arrived(block, order, d):
        arrived(wk.at[block, across_z(1), direct_rows(d), :], wx_r.at[order - 1])

    group_rows = pl.ds(pl.multiple_of(within, STATE), STATE)
    smsg[0:STATE, :] = st_s[group_rows, :].astype(BF16)
    smsg[STATE : STATE + 16, :] = jnp.concatenate([dec_s[...]] * 2, axis=0).astype(BF16)
    state_copies = [
        remote(smsg, srecv.at[k], state_s.at[k], state_r.at[k], ((e + 1 + k) % n_ep, t))
        for k in range(n_ep - 1)
    ]
    for k, copy in enumerate(state_copies):
        pl.when(e + 1 + k < n_ep)(copy.start)
    get_eg.wait()
    get_eu.wait()
    get_ed.wait()
    weight_along_z(z_order[-1])
    share_tokens(1, [0])
    experts(e, 0)
    share_tokens(1, [1])

    def order_of(way, d):
        if d == half_ring:
            return 2 * d - 1
        if d == 0:
            return 0
        return 2 * d - 1 + way

    def partner_sum(block, order):
        arrived(precv.at[block], pd_r.at[order])

    keep = feats * n_z
    keep_half = keep // 2

    def ring_sum(d, way):
        block = at_ring(d if way == 0 else -d)
        if d == half_ring:
            cols = pl.ds(way * keep_half, keep_half)
            value = pmine[block, :, cols].astype(F32) + precv[block, :, cols].astype(F32)
            pmine[block, :, cols] = value.astype(BF16)
            view = pmine.at[block, :, cols]
            send(
                view, rsrecv.at[way, d - 1, :, cols], rs_s.at[way, d - 1], rs_r.at[way, d - 1], toward[way]
            )
            return
        last = d == half_ring - 1
        cols = pl.ds(way * keep_half, keep_half) if last else pl.ds(0, keep)
        arrived(rsrecv.at[way, d, :, cols], rs_r.at[way, d])
        for k in reversed(range(n_z)):
            at = chunk_of(k)
            pmine[block, :, at] = (
                pmine[block, :, at].astype(F32)
                + precv[block, :, at].astype(F32)
                + rsrecv[way, d, :, at].astype(F32)
            ).astype(BF16)
            if d == 1:
                view = rsrecv.at[way, 0, :, at]
                send(pmine.at[block, :, at], view, rsl_s.at[way, k], rsl_r.at[way, k], toward[way])
        if d > 1:
            send(
                pmine.at[block], rsrecv.at[way, d - 1], rs_s.at[way, d - 1], rs_r.at[way, d - 1], toward[way]
            )

    def chunk_of(k):
        return pl.ds(pl.multiple_of(across_z(k) * feats, feats), feats)

    ent[...] = jnp.zeros_like(ent)
    for k in reversed(range(n_ep - 1)):

        @pl.when(e > k)
        def _(k=k):
            arrived(srecv.at[k], state_r.at[k])
            before = ent[group_rows, :]
            gone = srecv[k, STATE : STATE + 16, :].astype(F32)[0:1, :]
            ent[group_rows, :] = before * gone + srecv[k, 0:STATE, :].astype(F32)

    get_gate.wait()
    head_lane = lax.broadcasted_iota(jnp.int32, (1, width), 1) // STATE
    d_row = jnp.zeros((1, width), F32)
    for h in range(heads):
        d_row = jnp.where(head_lane == h, dscale[h], d_row)
    g_row = gnorm[...].astype(F32).reshape(1, width)
    row_id = lax.broadcasted_iota(jnp.int32, (BLOCK, BLOCK), 0)
    col_id = lax.broadcasted_iota(jnp.int32, (BLOCK, BLOCK), 1)
    same_head = (
        lax.broadcasted_iota(jnp.int32, (width, width), 0) // STATE
        == lax.broadcasted_iota(jnp.int32, (width, width), 1) // STATE
    )
    mean_of = jnp.where(same_head, 1.0 / STATE, 0.0).astype(BF16)

    def second_pass(k):
        rows = pl.ds(pl.multiple_of(k * BLOCK, BLOCK), BLOCK)
        xs_f = xs_s[rows, :].astype(F32)
        bs = bc_s[rows, pl.ds(0, LANES)]
        cs = bc_s[rows, pl.ds(LANES, LANES)]
        row_q = rows_s[k]
        cols = jnp.transpose(row_q)
        scores = dot(cs, bs, (((1,), (1,)), ((), ())))
        x_dt = (xs_f * spread(cols, 8)).astype(BF16)
        inner = []
        for j in range(width // LANES):
            both = []
            for h in (2 * j, 2 * j + 1):
                diff = cols[:, h : h + 1] - row_q[h : h + 1, :]
                link = jnp.exp(jnp.where(row_id >= col_id, diff, -1e30))
                both.append(dot((scores * link).astype(BF16), x_dt[:, j * LANES : (j + 1) * LANES]))
            inner.append(jnp.where(lane < STATE, both[0], both[1]))
        inner = jnp.concatenate(inner, axis=1) if len(inner) > 1 else inner[0]
        prev = prev_s[k] + ent[...] * dpre_s[k, 0:1, :]
        carried = dot(cs, prev.astype(BF16)) * spread(cols, 24)
        gated = (inner + carried + d_row * xs_f) * silu(gate[rows, :].astype(F32))
        square = gated * gated
        high = square.astype(BF16)
        low = (square - high.astype(F32)).astype(BF16)
        mean = dot(high, mean_of) + dot(low, mean_of)
        mixed[rows, :] = (gated * lax.rsqrt(mean + EPS) * g_row).astype(BF16)

    chip_rows = rows_dev * CORES
    per_chip = chip_rows // BLOCK

    def mix_for(k):
        target = across_z(k)

        def body(i, carry):
            second_pass(target * per_chip + i)
            return carry

        lax.fori_loop(0, per_chip, body, 0)
        view = mixed.at[pl.ds(pl.multiple_of(target * chip_rows, chip_rows), chip_rows), :]
        if k:
            send(view, mrecv.at[z], a2a_s.at[k - 1], a2a_r.at[k - 1], z_device(k))
        else:
            own = pl.ds(pl.multiple_of(z * chip_rows, chip_rows), chip_rows)
            mrecv[z] = mixed[own, :]

    def ring_step(d):
        for way in range(2):
            partner_sum(at_ring(d if way == 0 else -d), order_of(1 - way, d))
            ring_sum(d, way)

    mixes = [k for k in range(2, n_z)] + [1, 0]
    waiting = list(z_order)
    mix_for(mixes.pop(0))
    share_tokens(1, [2])
    first_weight(waiting.pop(0))
    first_weight(waiting.pop(0))
    for d in range(1, half_ring):
        for way in range(2):
            direct_weight(at_ring(-d if way == 0 else d), order_of(way, d), d)
    direct_weight(at_ring(half_ring), order_of(0, half_ring), half_ring)
    for k in range(1, n_ep):
        arrived(wts.at[(e - k + n_ep) % n_ep], wts_r.at[k - 1])
    for way in range(2):
        shared_tokens(way, 1)
    for d in range(1, half_ring):
        for way in range(2):
            experts(at_ring(-d if way == 0 else d), order_of(way, d))
            if way == 0:
                share_tokens(d + 1, pieces_of(d + 1))
        for way in range(2):
            shared_tokens(way, d + 1)
    experts(at_ring(half_ring), order_of(0, half_ring))
    partner_sum(at_ring(half_ring), order_of(0, half_ring))
    for way in range(2):
        ring_sum(half_ring, way)
    mix_for(mixes.pop(0))
    while waiting:
        first_weight(waiting.pop(0))
    for k in mixes:
        mix_for(k)
    for d in range(half_ring - 1, 0, -1):
        ring_step(d)

    for d in range(1, half_ring):
        for k in z_order:
            pass_weight(d, k)

    def own_sum(k):
        at = chunk_of(k)
        for way in range(2):
            arrived(rsrecv.at[way, 0, :, at], rsl_r.at[way, k])
        return (
            pmine[e, :, at].astype(F32)
            + precv[e, :, at].astype(F32)
            + rsrecv[0, 0, :, at].astype(F32)
            + rsrecv[1, 0, :, at].astype(F32)
        )

    partner_sum(e, 0)
    for k in reversed(range(1, n_z)):
        zsend[k - 1] = own_sum(k).astype(BF16)
        send(zsend.at[k - 1], zrecv.at[k - 1], zs_s.at[k - 1], zs_r.at[k - 1], z_device(k))
    eown[...] = own_sum(0)

    for k in range(1, n_z):
        arrived(mrecv.at[across_z(k)], a2a_r.at[k - 1])
    for copy in get_w:
        copy.wait()

    def rows_of(core):
        return pl.ds(pl.multiple_of(core * rows_dev, rows_dev), rows_dev)

    def product(core, block):
        total = dot(mrecv[0, rows_of(core), :], wk[block, 0])
        for k in range(1, n_z):
            total = total + dot(mrecv[k, rows_of(core), :], wk[block, k])
        return total

    def give(order):
        send(pjsend.at[order], pjrecv.at[order], pj_s.at[order], pj_r.at[order], partner)

    def project(block, order):
        pjsend[order] = product(1 - c, block).astype(BF16)
        give(order)
        pjown[order] = product(c, block)

    def project_late(block, order):
        both = (c, 1 - c)
        for core, total in zip(both, (pjown.at[order], pjlast)):
            total[...] = dot(mrecv[z, rows_of(core), :], wk[block, z])
        for k in z_order:
            for way in range(2):
                weight_arrived(way, half_ring, k)
            if k == 1:
                direct_arrived(block, order, half_ring)
            place = across_z(k)
            if k == z_order[-1]:
                total = pjlast[...] + dot(mrecv[place, rows_of(1 - c), :], wk[block, place])
                pjsend[order] = total.astype(BF16)
                give(order)
                pjown[order] += dot(mrecv[place, rows_of(c), :], wk[block, place])
            else:
                for core, total in zip(both, (pjown.at[order], pjlast)):
                    total[...] += dot(mrecv[place, rows_of(core), :], wk[block, place])

    puts = []

    def put(src, dst, index):
        copy = pltpu.make_async_copy(src, dst, ld.at[index])
        copy.start()
        puts.append(copy)

    def finish(block, order):
        arrived(pjrecv.at[order], pj_r.at[order])
        result[order] = (pjown[order] + pjrecv[order].astype(F32)).astype(BF16)
        cols = pl.ds(pl.multiple_of(block * part, part), part)
        put(result.at[order], out.at[:, cols], order)

    project(e, 0)
    done = [(e, 0)]
    for d in range(1, half_ring):
        for way in range(2):
            block = at_ring(-d if way == 0 else d)
            direct_arrived(block, order_of(way, d), d)
            project(block, order_of(way, d))
            done.append((block, order_of(way, d)))

    total = eown[...]
    for k in range(1, n_z):
        arrived(zrecv.at[k - 1], zs_r.at[k - 1])
        total = total + zrecv[k - 1].astype(F32)
    eresult[...] = total.astype(BF16)
    put(eresult, eout, n_ep)

    for block, order in done:
        finish(block, order)
    project_late(at_ring(half_ring), order_of(0, half_ring))
    finish(at_ring(half_ring), order_of(0, half_ring))

    for copy in pending:
        copy.wait_send()
    for copy in puts:
        copy.wait()

    @pl.when(e < n_ep - 1)
    def _():
        for copy in halo:
            copy.wait_send()

    for k, copy in enumerate(state_copies):
        pl.when(e + 1 + k < n_ep)(copy.wait_send)


def hand_over_kernel(chunks, a_in, b_in, a_out, b_out, a, b, sems):
    rows = a.shape[0] // chunks
    moves = [(a_in.at[pl.ds(i * rows, rows)], a.at[pl.ds(i * rows, rows)], a_out.at[pl.ds(i * rows, rows)]) for i in range(chunks)]
    moves.append((b_in, b, b_out))
    reads = [pltpu.make_async_copy(m[0], m[1], sems.at[0, i]) for i, m in enumerate(moves)]
    writes = [pltpu.make_async_copy(m[1], m[2], sems.at[1, i]) for i, m in enumerate(moves)]
    for copy in reads:
        copy.start()
    for read, write in zip(reads, writes):
        read.wait()
        write.start()
    for copy in writes:
        copy.wait()


def hand_over(a, b):
    chunks = 8
    anywhere = pl.BlockSpec(memory_space=pl.ANY)
    return pl.pallas_call(
        functools.partial(hand_over_kernel, chunks),
        out_shape=(jax.ShapeDtypeStruct(a.shape, a.dtype), jax.ShapeDtypeStruct(b.shape, b.dtype)),
        in_specs=[anywhere] * 2,
        out_specs=(anywhere, anywhere),
        scratch_shapes=[
            pltpu.VMEM(a.shape, a.dtype),
            pltpu.VMEM(b.shape, b.dtype),
            pltpu.SemaphoreType.DMA((2, chunks + 1)),
        ],
        name="hand_over",
    )(a, b)


def fused(n_ep, n_tp, args):
    (
        x,
        gate_logits,
        b_map,
        c_map,
        xtaps,
        btaps,
        ctaps,
        step,
        lograte,
        extra,
        dscale,
        gnorm,
        wout,
        tokens,
        pnorm,
        group_cols,
        expert_cols,
        routes,
        eg,
        eu,
        ed,
    ) = args
    operands = (
        x,
        gate_logits,
        b_map,
        c_map,
        wout,
        tokens,
        eg[0],
        eu[0],
        ed[0],
        xtaps,
        btaps,
        ctaps,
        step,
        extra,
        lograte,
        dscale,
        gnorm,
        pnorm,
        group_cols.T,
        expert_cols.T,
        routes.T,
    )
    n_z = n_tp // CORES
    half_ring = n_ep // 2
    length, width = x.shape
    heads = dscale.shape[0]
    nblk = length // BLOCK
    n_tok, depth = tokens.shape
    feats = depth // n_tp
    ff = eg.shape[2]
    rows_w, cols_w = wout.shape
    part = cols_w // n_ep
    rows_dev = length // n_tp
    chip_rows = rows_dev * CORES
    w_rows = -(-expert_cols.shape[1] // 8) * 8
    slots = max(2, min(n_ep, 16 // n_ep))
    keep = n_z * feats
    anywhere = pl.BlockSpec(memory_space=pl.ANY)
    dma = pltpu.SemaphoreType.DMA
    scratch = [
        (pltpu.SMEM if v.dtype == F32 and v.ndim == 1 else pltpu.VMEM)(v.shape, v.dtype)
        for v in operands[9:]
    ]
    scratch += [
        pltpu.VMEM((length + HALO, width), BF16),
        pltpu.VMEM((length + HALO, 2 * LANES), BF16),
        pltpu.VMEM((length, width), BF16),
        pltpu.VMEM((depth, ff), BF16),
        pltpu.VMEM((depth, ff), BF16),
        pltpu.VMEM((ff, depth), BF16),
        pltpu.VMEM((n_ep, n_z, rows_w, part), BF16),
        pltpu.VMEM((n_ep, n_tok, depth), BF16),
        pltpu.VMEM((n_ep, w_rows, n_tok), F32),
        pltpu.VMEM((n_tok, ff), BF16),
        pltpu.VMEM((slots, n_tok, keep), BF16),
        pltpu.VMEM((n_ep, n_tok, keep), BF16),
        pltpu.VMEM((n_ep, n_tok, keep), BF16),
        pltpu.VMEM((2, half_ring, n_tok, keep), BF16),
        pltpu.VMEM((n_z - 1, n_tok, feats), BF16),
        pltpu.VMEM((n_z - 1, n_tok, feats), BF16),
        pltpu.VMEM((length, width), BF16),
        pltpu.VMEM((length, 2 * LANES), BF16),
        pltpu.VMEM((nblk, BLOCK, BLOCK), F32),
        pltpu.VMEM((nblk, LANES, width), F32),
        pltpu.VMEM((nblk, 8, width), F32),
        pltpu.VMEM((LANES, width), F32),
        pltpu.VMEM((8, width), F32),
        pltpu.VMEM((STATE + 16, width), BF16),
        pltpu.VMEM((n_ep - 1, STATE + 16, width), BF16),
        pltpu.VMEM((LANES, width), F32),
        pltpu.VMEM((length, width), BF16),
        pltpu.VMEM((n_z, chip_rows, width), BF16),
        pltpu.VMEM((n_ep, rows_dev, part), BF16),
        pltpu.VMEM((n_ep, rows_dev, part), F32),
        pltpu.VMEM((rows_dev, part), F32),
        pltpu.VMEM((n_ep, rows_dev, part), BF16),
        pltpu.VMEM((n_ep, rows_dev, part), BF16),
        pltpu.VMEM((n_tok, feats), BF16),
        pltpu.VMEM((n_tok, feats), F32),
        dma((21 + n_ep,)),
        dma((3,)),
        dma((3,)),
    ]
    for shape in (
        (2, half_ring, 3),
        (2, half_ring, 3),
        (n_ep - 1,),
        (n_z - 1,),
        (2, half_ring, n_z - 1),
        (n_ep - 1,),
        (n_ep - 1,),
        (n_ep,),
        (2, half_ring),
        (2, n_z),
        (n_z - 1,),
        (n_z - 1,),
        (n_ep,),
    ):
        scratch += [dma(shape), dma(shape)]
    mixer_out, experts_out = pl.pallas_call(
        functools.partial(kernel, n_ep, n_tp),
        out_shape=(
            jax.ShapeDtypeStruct((rows_dev, cols_w), BF16),
            jax.ShapeDtypeStruct((n_tok, feats), BF16),
        ),
        in_specs=[anywhere] * len(operands),
        out_specs=(anywhere, anywhere),
        scratch_shapes=scratch,
        name="fused",
        compiler_params=pltpu.CompilerParams(
            collective_id=0, has_side_effects=True, vmem_limit_bytes=67_000_000
        ),
    )(*operands)
    return hand_over(mixer_out, experts_out)


def solution(mesh):
    n_ep, n_tp = mesh.shape["ep"], mesh.shape["tp"]
    in_specs = (
        P("ep", "tp"),
        P("ep", "tp"),
        P("ep", None),
        P("ep", None),
        P(None, "tp"),
        P(),
        P(),
        P("tp", "ep"),
        P("tp"),
        P("tp", "ep"),
        P("tp"),
        P("tp"),
        P("tp", None),
        P("ep", None),
        P(),
        P(),
        P(),
        P("ep", None),
        P("ep", None, "tp"),
        P("ep", None, "tp"),
        P("ep", "tp", None),
    )
    out_specs = (P(("ep", "tp"), None), P("ep", "tp"))
    return jax.shard_map(
        lambda *args: fused(n_ep, n_tp, args),
        mesh=mesh,
        in_specs=in_specs,
        out_specs=out_specs,
        check_vma=False,
    )
```

```python
import functools
import math

import jax
import jax.numpy as jnp
from jax import lax
from jax.experimental import pallas as pl
from jax.experimental.pallas import tpu as pltpu
from jax.sharding import PartitionSpec as P

STATE = 64
GROUPS = 4
HEADS = 32
BLOCK = 128
CORES = 2
LANES = 128
HALO = 16
EPS = 1e-6
MESH = pl.DeviceIdType.MESH
F32 = jnp.float32
BF16 = jnp.bfloat16


def snake(i, n):
    w = math.isqrt(n)
    y, x = i // w, i % w
    odd = y % 2
    return y * w + x * (1 - 2 * odd) + odd * (w - 1)


def silu(v):
    return v / (1.0 + jnp.exp(-v))


def dot(a, b, dims=(((1,), (0,)), ((), ()))):
    return lax.dot_general(a, b, dims, preferred_element_type=F32)


def kernel(
    n_ep,
    n_tp,
    x_hbm,
    gate_hbm,
    b_hbm,
    c_hbm,
    wout_hbm,
    tok_hbm,
    eg_hbm,
    eu_hbm,
    ed_hbm,
    xtaps_hbm,
    btaps_hbm,
    ctaps_hbm,
    step_hbm,
    extra_hbm,
    lograte_hbm,
    dscale_hbm,
    gnorm_hbm,
    pnorm_hbm,
    grouter_hbm,
    erouter_hbm,
    routes_hbm,
    out,
    eout,
    xtaps,
    btaps,
    ctaps,
    step,
    extra,
    lograte,
    dscale,
    gnorm,
    pnorm,
    grouter,
    erouter,
    routes,
    xpad,
    bcpad,
    gate,
    eg,
    eu,
    ed,
    wk,
    rows_tok,
    wts,
    hid,
    psend,
    pmine,
    precv,
    rsrecv,
    zsend,
    zrecv,
    xs_s,
    bc_s,
    rows_s,
    prev_s,
    dpre_s,
    st_s,
    dec_s,
    smsg,
    srecv,
    ent,
    mixed,
    mrecv,
    pjsend,
    pjown,
    pjlast,
    pjrecv,
    eown,
    pool,
    halo_s,
    halo_r,
    state_s,
    state_r,
    tok_r,
    tokp_r,
    wts_r,
    wz_r,
    wr_r,
    wx_r,
    pd_r,
    rs_r,
    rsl_r,
    zs_r,
    a2a_r,
    pj_r,
):
    n_z = n_tp // CORES
    half_ring = n_ep // 2
    e = lax.axis_index("ep")
    t = lax.axis_index("tp")
    c = t % CORES
    z = t // CORES
    ring = snake(e, n_ep)
    partner = (e, t + 1 - 2 * c)

    def across_z(k):
        place, bit = 0, 1
        while bit < n_z:
            own = z // bit % 2
            place = place + bit * ((1 - own) if k & bit else own)
            bit *= 2
        return place

    def z_device(k):
        return (e, CORES * across_z(k) + c)

    def at_ring(offset):
        return snake((ring + offset + n_ep) % n_ep, n_ep)

    next_ep, prev_ep = at_ring(1), at_ring(-1)
    toward = ((next_ep, t), (prev_ep, t))
    length, width = x_hbm.shape
    heads = width // STATE
    nblk = length // BLOCK
    group = t * heads // (HEADS // GROUPS)
    pair = group * STATE // LANES
    within = group * STATE % LANES
    n_tok, depth = tok_hbm.shape
    half = n_tok // CORES
    quarter = half // 2
    feats = depth // n_tp
    ff = eg_hbm.shape[1]
    rows_w = wout_hbm.shape[0]
    part = wout_hbm.shape[1] // n_ep
    rows_dev = out.shape[0]
    pending = []

    def remote(src, dst, send, recv, device):
        return pltpu.make_async_remote_copy(
            src_ref=src, dst_ref=dst, send_sem=send, recv_sem=recv, device_id=device, device_id_type=MESH
        )

    free = list(range(pool.shape[0]))

    def send_done(entry):
        entry[0].wait_send()
        free.append(entry[1])
        pending[:] = [one for one in pending if one is not entry]

    def send(src, dst, recv_sem, device):
        if not free:
            send_done(pending[0])
        index = free.pop(0)
        copy = remote(src, dst, pool.at[index], recv_sem, device)
        copy.start()
        entry = (copy, index)
        pending.append(entry)
        return entry

    def arrived(view, sem):
        remote(view, view, sem, sem, partner).wait_recv()

    def local(src, dst):
        index = free.pop(0)
        copy = pltpu.make_async_copy(src, dst, pool.at[index])
        copy.start()
        return copy, index

    def here(*entries):
        for copy, index in entries:
            copy.wait()
            free.append(index)

    barrier = pltpu.get_barrier_semaphore()
    peers = 0
    for k in range(1, n_ep):
        pl.semaphore_signal(barrier, inc=1, device_id=((e + k) % n_ep, t), device_id_type=MESH)
        peers += 1
    for k in range(1, n_z):
        pl.semaphore_signal(barrier, inc=1, device_id=z_device(k), device_id_type=MESH)
        peers += 1
    pl.semaphore_signal(barrier, inc=1, device_id=partner, device_id_type=MESH)
    peers += 1

    get_tok = [
        local(tok_hbm.at[rows], rows_tok.at[e, rows])
        for i, rows in enumerate(
            pl.ds(pl.multiple_of(core * (tok_hbm.shape[0] // CORES), 32), tok_hbm.shape[0] // CORES)
            for core in (c, 1 - c)
        )
    ]
    get_pnorm = local(pnorm_hbm, pnorm)
    get_eg = local(eg_hbm, eg)
    get_eu = local(eu_hbm, eu)
    get_ed = local(ed_hbm, ed)
    lane_b = pl.ds(pl.multiple_of(pair * LANES, LANES), LANES)
    get_x = local(x_hbm, xpad.at[pl.ds(HALO, length)])
    get_b = local(b_hbm.at[:, lane_b], bcpad.at[pl.ds(HALO, length), pl.ds(0, LANES)])
    get_c = local(c_hbm.at[:, lane_b], bcpad.at[pl.ds(HALO, length), pl.ds(LANES, LANES)])
    get_gate = local(gate_hbm, gate)
    get_w = [
        local(wout_hbm.at[:, pl.ds(q * part, part)], wk.at[q, z]) for q in range(n_ep)
    ]

    get_small = [
        local(src, dst)
        for i, (src, dst) in enumerate(
            (
                (grouter_hbm, grouter),
                (erouter_hbm, erouter),
                (routes_hbm, routes),
                (step_hbm, step),
                (extra_hbm, extra),
                (lograte_hbm, lograte),
                (xtaps_hbm, xtaps),
                (btaps_hbm, btaps),
                (ctaps_hbm, ctaps),
                (dscale_hbm, dscale),
                (gnorm_hbm, gnorm),
            )
        )
    ]

    here(get_pnorm)
    here(get_tok[0])
    scale = pnorm[...].astype(F32).reshape(1, depth)

    def norm_rows(i, carry):
        rows = pl.ds(pl.multiple_of(i * 32, 32), 32)
        v = rows_tok[e, rows, :].astype(F32)
        v = v * lax.rsqrt(jnp.mean(v * v, axis=-1, keepdims=True) + EPS) * scale
        rows_tok[e, rows, :] = v.astype(BF16)
        return carry

    steps = half // 32
    lax.fori_loop(c * steps, c * steps + steps, norm_rows, 0)

    pl.semaphore_wait(barrier, peers)

    def tok_view(core, way, d, piece):
        block = at_ring(-d if way == 0 else d)
        if piece == 0:
            first, count = core * half + way * quarter, quarter
        else:
            first, count = core * half + (1 - way) * quarter, quarter
        return rows_tok.at[block, pl.ds(pl.multiple_of(first, count), count), :]

    def pieces_of(d):
        return range(1 if d == half_ring else 2)

    def send_tokens(way, d, piece):
        view = tok_view(c, way, d - 1, piece)
        send(view, view, tok_r.at[way, d - 1, piece], toward[way])

    def share_tokens(d, pieces):
        for piece in pieces:
            for way in range(2):
                view = tok_view(c, way, d, piece)
                arrived(view, tok_r.at[way, d - 1, piece])
                if d < half_ring and piece in pieces_of(d + 1):
                    send_tokens(way, d + 1, piece)
                send(view, view, tokp_r.at[way, d - 1, piece], partner)

    def shared_tokens(way, d):
        for piece in pieces_of(d):
            arrived(tok_view(1 - c, way, d, piece), tokp_r.at[way, d - 1, piece])

    tail_rows = pl.ds(length - HALO, HALO)
    head_rows = pl.ds(0, HALO)
    halo = [
        remote(src, dst, halo_s.at[i], halo_r.at[i], ((e + 1) % n_ep, t))
        for i, (src, dst) in enumerate(
            (
                (x_hbm.at[tail_rows], xpad.at[head_rows]),
                (b_hbm.at[tail_rows, lane_b], bcpad.at[head_rows, pl.ds(0, LANES)]),
                (c_hbm.at[tail_rows, lane_b], bcpad.at[head_rows, pl.ds(LANES, LANES)]),
            )
        )
    ]

    @pl.when(e < n_ep - 1)
    def _():
        for copy in halo:
            copy.start()

    @pl.when(e == 0)
    def _():
        xpad[head_rows, :] = jnp.zeros((HALO, width), BF16)
        bcpad[head_rows, :] = jnp.zeros((HALO, 2 * LANES), BF16)

    for piece in pieces_of(1):
        for way in range(2):
            send_tokens(way, 1, piece)

    mine = pl.ds(pl.multiple_of(e * part, part), part)
    z_order = sorted(range(1, n_z), key=lambda k: (k != 1, -k))

    def weight_along_z(k):
        send(wout_hbm.at[:, mine], wk.at[e, z], wz_r.at[k - 1], z_device(k))

    for k in z_order[:-1]:
        weight_along_z(k)

    here(get_tok[1])
    here(*get_small)
    lax.fori_loop((1 - c) * steps, (1 - c) * steps + steps, norm_rows, 0)

    for way in range(2):
        rest = pl.ds((1 - way) * (n_z * feats // 2), n_z * feats // 2)
        rsrecv[way, half_ring - 1, :, rest] = jnp.zeros((n_tok, n_z * feats // 2), BF16)

    n_experts, n_grp = erouter.shape[0], grouter.shape[0]
    over_rows = (((1,), (1,)), ((), ()))
    logits = dot(erouter[...], rows_tok[e], over_rows)
    expert_logit = [logits[i : i + 1, :] for i in range(n_experts)]
    logits = dot(grouter[...], rows_tok[e], over_rows)
    per_group = n_experts // n_grp
    group_logit = [logits[i : i + 1, :] for i in range(n_grp)]

    def log_softmax(rows):
        top = functools.reduce(jnp.maximum, rows)
        norm = jnp.log(functools.reduce(jnp.add, [jnp.exp(v - top) for v in rows]))
        return [v - top - norm for v in rows]

    group_lp = log_softmax(group_logit)
    total_lp = []
    for i in range(n_grp):
        inner = log_softmax(expert_logit[i * per_group : (i + 1) * per_group])
        total_lp += [group_lp[i] + v for v in inner]
    picks = [routes[k : k + 1, :] for k in range(2)]
    chosen = []
    for k in range(2):
        value = jnp.zeros_like(total_lp[0])
        for i in range(n_experts):
            value = jnp.where(picks[k] == i, total_lp[i], value)
        chosen.append(value)
    top = jnp.maximum(chosen[0], chosen[1])
    share = [jnp.exp(v - top) for v in chosen]
    inv = 1.0 / (share[0] + share[1])
    share = [v * inv for v in share]
    wts[e] = jnp.zeros(wts.shape[1:], F32)
    for i in range(n_experts):
        wts[e, i : i + 1, :] = jnp.where(picks[0] == i, share[0], 0.0) + jnp.where(
            picks[1] == i, share[1], 0.0
        )
    for k in range(1, n_ep):
        send(wts.at[e], wts.at[e], wts_r.at[k - 1], ((e + k) % n_ep, t))

    slots = psend.shape[0]
    to_partner = {}

    def experts(block, order):
        wrow = wts[block, pl.ds(e, 1), :]
        wcol = jnp.transpose(jnp.broadcast_to(wrow, (LANES, n_tok)))
        wide = 256
        wcol = jnp.concatenate([wcol] * (wide // LANES), axis=1)

        def up(j, carry):
            cols = pl.ds(pl.multiple_of(j * wide, wide), wide)
            g = dot(rows_tok[block], eg[:, cols])
            u = dot(rows_tok[block], eu[:, cols])
            hid[:, cols] = (silu(g) * u * wcol).astype(BF16)
            return carry

        lax.fori_loop(0, ff // wide, up, 0)
        slot = order % slots
        if order >= slots:
            earlier = to_partner[order - slots]
            if any(one is earlier for one in pending):
                send_done(earlier)

        def down(into, core):
            for k in range(n_z):
                at = pl.ds(k * feats, feats)
                cols = pl.ds(pl.multiple_of((CORES * k + core) * feats, feats), feats)
                into[:, at] = dot(hid[...], ed[:, cols]).astype(BF16)

        down(psend.at[slot], 1 - c)
        to_partner[order] = send(
            psend.at[slot], precv.at[block], pd_r.at[order], partner
        )
        down(pmine.at[block], c)

    lane = lax.broadcasted_iota(jnp.int32, (1, LANES), 1)
    head_row = lax.broadcasted_iota(jnp.int32, (heads, 1), 0)
    rate = jnp.zeros((heads, 1), F32)
    for h in range(heads):
        rate = jnp.where(head_row == h, lograte[h], rate)
    rate = jnp.exp(rate)
    for k in range(nblk):
        at = pl.ds(k * BLOCK, BLOCK)
        v = step[:, at]
        dt = jnp.maximum(v, 0.0) + jnp.log(1.0 + jnp.exp(-jnp.abs(v)))
        cum = extra[:, at] - dt * rate
        hop = 1
        while hop < BLOCK:
            cum = cum + jnp.where(lane >= hop, pltpu.roll(cum, hop, 1), 0.0)
            hop *= 2
        grown = jnp.exp(cum)
        left = jnp.exp(cum[:, BLOCK - 1 :] - cum) * dt
        rows_s[k, 0:heads, :] = cum
        rows_s[k, 8 : 8 + heads, :] = dt
        rows_s[k, 16 : 16 + heads, :] = left
        rows_s[k, 24 : 24 + heads, :] = grown

    def spread(cols, first):
        pieces = []
        for j in range(width // LANES):
            low = cols[:, first + 2 * j : first + 2 * j + 1]
            high = cols[:, first + 2 * j + 1 : first + 2 * j + 2]
            pieces.append(jnp.where(lane < STATE, low, high))
        return jnp.concatenate(pieces, axis=1) if len(pieces) > 1 else pieces[0]

    here(get_x)
    here(get_b)
    here(get_c)

    @pl.when(e > 0)
    def _():
        for copy in halo:
            copy.wait_recv()

    x_w = xtaps[...].astype(F32)
    bc_w = jnp.concatenate([btaps[:, lane_b], ctaps[:, lane_b]], axis=1).astype(F32)
    lane2 = lax.broadcasted_iota(jnp.int32, (1, 2 * LANES), 1) % LANES
    in_group = (lane2 >= within) & (lane2 < within + STATE)
    taps = x_w.shape[0]

    def conv(ref, w, k):
        v = ref[pl.ds(pl.multiple_of(k * BLOCK, BLOCK), BLOCK + HALO), :].astype(F32)
        total = v[HALO:] * w[taps - 1 :]
        for j in range(taps - 1):
            total = total + pltpu.roll(v, taps - 1 - j, 0)[HALO:] * w[j : j + 1]
        return silu(total)

    st_s[...] = jnp.zeros_like(st_s)
    dec_s[...] = jnp.ones_like(dec_s)

    def first_pass(k, carry):
        rows = pl.ds(pl.multiple_of(k * BLOCK, BLOCK), BLOCK)
        xs = conv(xpad, x_w, k).astype(BF16)
        bc = jnp.where(in_group, conv(bcpad, bc_w, k), 0.0).astype(BF16)
        xs_s[rows, :] = xs
        bc_s[rows, :] = bc
        cols = jnp.transpose(rows_s[k])
        xw = (xs.astype(F32) * spread(cols, 16)).astype(BF16)
        block_state = dot(bc[:, :LANES], xw, (((0,), (0,)), ((), ())))
        gone = spread(cols[BLOCK - 8 :, :], 24)[7:8, :]
        prev_s[k] = st_s[...]
        dpre_s[k] = dec_s[...]
        st_s[...] = st_s[...] * gone + block_state
        dec_s[...] = dec_s[...] * gone
        return carry

    lax.fori_loop(0, nblk, first_pass, 0)

    def order_of(way, d):
        if d == half_ring:
            return 2 * d - 1
        if d == 0:
            return 0
        return 2 * d - 1 + way

    half_w = rows_w // 2

    def weight_view(block, way, k, d):
        slab = wk.at[block, across_z(k)]
        if d == half_ring:
            return slab.at[pl.ds(way * half_w, half_w), :]
        return slab.at[pl.ds(0, half_w), :] if k == 1 else slab

    def on_ring(d, k):
        return k != 1 or d < half_ring

    def send_weight(way, d, k):
        if on_ring(d, k):
            view = weight_view(at_ring(-(d - 1) if way == 0 else d - 1), way, k, d)
            send(view, view, wr_r.at[way, d - 1, k - 1], toward[way])

    def first_weight(k):
        arrived(wk.at[e, across_z(k)], wz_r.at[k - 1])
        for way in range(2):
            send_weight(way, 1, k)

    def weight_arrived(way, d, k):
        if on_ring(d, k):
            view = weight_view(at_ring(-d if way == 0 else d), way, k, d)
            arrived(view, wr_r.at[way, d - 1, k - 1])

    def pass_weight(d, k):
        for way in range(2):
            weight_arrived(way, d, k)
            send_weight(way, d + 1, k)

    def direct_rows(d):
        return pl.ds(0, rows_w) if d == half_ring else pl.ds(half_w, rows_w - half_w)

    def direct_weights():
        entries = []
        targets = [(way, d) for d in range(1, half_ring) for way in range(2)] + [(0, half_ring)]
        for way, d in targets:
            block = at_ring(-d if way == 0 else d)
            cols = pl.ds(pl.multiple_of(block * part, part), part)
            index = free.pop(0)
            copy = remote(
                wout_hbm.at[direct_rows(d), cols],
                wk.at[block, z, direct_rows(d), :],
                pool.at[index],
                wx_r.at[order_of(way, d) - 1],
                z_device(1),
            )
            entries.append((copy, index))
        return entries

    two_sided = (z > 0) & (z < n_z - 1)

    def direct_arrived(block, order, d):
        arrived(wk.at[block, across_z(1), direct_rows(d), :], wx_r.at[order - 1])

    group_rows = pl.ds(pl.multiple_of(within, STATE), STATE)
    smsg[0:STATE, :] = st_s[group_rows, :].astype(BF16)
    smsg[STATE : STATE + 16, :] = jnp.concatenate([dec_s[...]] * 2, axis=0).astype(BF16)
    state_copies = [
        remote(smsg, srecv.at[k], state_s.at[k], state_r.at[k], ((e + 1 + k) % n_ep, t))
        for k in range(n_ep - 1)
    ]
    for k, copy in enumerate(state_copies):
        pl.when(e + 1 + k < n_ep)(copy.start)
    here(get_eg)
    here(get_eu)
    here(get_ed)
    weight_along_z(z_order[-1])
    direct = direct_weights()

    @pl.when(two_sided)
    def _():
        for copy, _index in direct:
            copy.start()

    share_tokens(1, [0])
    experts(e, 0)
    share_tokens(1, [1])

    def partner_sum(block, order):
        arrived(precv.at[block], pd_r.at[order])

    keep = feats * n_z
    keep_half = keep // 2

    def ring_sum(d, way):
        block = at_ring(d if way == 0 else -d)
        if d == half_ring:
            cols = pl.ds(way * keep_half, keep_half)
            value = pmine[block, :, cols].astype(F32) + precv[block, :, cols].astype(F32)
            pmine[block, :, cols] = value.astype(BF16)
            view = pmine.at[block, :, cols]
            send(
                view, rsrecv.at[way, d - 1, :, cols], rs_r.at[way, d - 1], toward[way]
            )
            return
        last = d == half_ring - 1
        cols = pl.ds(way * keep_half, keep_half) if last else pl.ds(0, keep)
        arrived(rsrecv.at[way, d, :, cols], rs_r.at[way, d])
        for k in reversed(range(n_z)):
            at = chunk_of(k)
            pmine[block, :, at] = (
                pmine[block, :, at].astype(F32)
                + precv[block, :, at].astype(F32)
                + rsrecv[way, d, :, at].astype(F32)
            ).astype(BF16)
            if d == 1:
                view = rsrecv.at[way, 0, :, at]
                send(pmine.at[block, :, at], view, rsl_r.at[way, k], toward[way])
        if d > 1:
            send(
                pmine.at[block], rsrecv.at[way, d - 1], rs_r.at[way, d - 1], toward[way]
            )

    def chunk_of(k):
        return pl.ds(pl.multiple_of(across_z(k) * feats, feats), feats)

    ent[...] = jnp.zeros_like(ent)
    for k in reversed(range(n_ep - 1)):

        @pl.when(e > k)
        def _(k=k):
            arrived(srecv.at[k], state_r.at[k])
            before = ent[group_rows, :]
            gone = srecv[k, STATE : STATE + 16, :].astype(F32)[0:1, :]
            ent[group_rows, :] = before * gone + srecv[k, 0:STATE, :].astype(F32)

    here(get_gate)
    head_lane = lax.broadcasted_iota(jnp.int32, (1, width), 1) // STATE
    d_row = jnp.zeros((1, width), F32)
    for h in range(heads):
        d_row = jnp.where(head_lane == h, dscale[h], d_row)
    g_row = gnorm[...].astype(F32).reshape(1, width)
    row_id = lax.broadcasted_iota(jnp.int32, (BLOCK, BLOCK), 0)
    col_id = lax.broadcasted_iota(jnp.int32, (BLOCK, BLOCK), 1)
    same_head = (
        lax.broadcasted_iota(jnp.int32, (width, width), 0) // STATE
        == lax.broadcasted_iota(jnp.int32, (width, width), 1) // STATE
    )
    mean_of = jnp.where(same_head, 1.0 / STATE, 0.0).astype(BF16)

    def second_pass(k):
        rows = pl.ds(pl.multiple_of(k * BLOCK, BLOCK), BLOCK)
        xs_f = xs_s[rows, :].astype(F32)
        bs = bc_s[rows, pl.ds(0, LANES)]
        cs = bc_s[rows, pl.ds(LANES, LANES)]
        row_q = rows_s[k]
        cols = jnp.transpose(row_q)
        scores = dot(cs, bs, (((1,), (1,)), ((), ())))
        x_dt = (xs_f * spread(cols, 8)).astype(BF16)
        inner = []
        for j in range(width // LANES):
            both = []
            for h in (2 * j, 2 * j + 1):
                diff = cols[:, h : h + 1] - row_q[h : h + 1, :]
                link = jnp.exp(jnp.where(row_id >= col_id, diff, -1e30))
                both.append(dot((scores * link).astype(BF16), x_dt[:, j * LANES : (j + 1) * LANES]))
            inner.append(jnp.where(lane < STATE, both[0], both[1]))
        inner = jnp.concatenate(inner, axis=1) if len(inner) > 1 else inner[0]
        prev = prev_s[k] + ent[...] * dpre_s[k, 0:1, :]
        carried = dot(cs, prev.astype(BF16)) * spread(cols, 24)
        gated = (inner + carried + d_row * xs_f) * silu(gate[rows, :].astype(F32))
        square = gated * gated
        high = square.astype(BF16)
        low = (square - high.astype(F32)).astype(BF16)
        mean = dot(high, mean_of) + dot(low, mean_of)
        mixed[rows, :] = (gated * lax.rsqrt(mean + EPS) * g_row).astype(BF16)

    chip_rows = rows_dev * CORES
    per_chip = chip_rows // BLOCK

    def mix_for(k):
        target = across_z(k)

        def body(i, carry):
            second_pass(target * per_chip + i)
            return carry

        lax.fori_loop(0, per_chip, body, 0)
        view = mixed.at[pl.ds(pl.multiple_of(target * chip_rows, chip_rows), chip_rows), :]
        if k:
            send(view, mrecv.at[z], a2a_r.at[k - 1], z_device(k))
        else:
            own = pl.ds(pl.multiple_of(z * chip_rows, chip_rows), chip_rows)
            mrecv[z] = mixed[own, :]

    def ring_step(d):
        for way in range(2):
            partner_sum(at_ring(d if way == 0 else -d), order_of(1 - way, d))
            ring_sum(d, way)

    mixes = [k for k in range(2, n_z)] + [1, 0]
    waiting = list(z_order)
    mix_for(mixes.pop(0))
    first_weight(waiting.pop(0))
    first_weight(waiting.pop(0))

    @pl.when(jnp.logical_not(two_sided))
    def _():
        for copy, _index in direct:
            copy.start()

    pending.extend(direct)
    for k in range(1, n_ep):
        arrived(wts.at[(e - k + n_ep) % n_ep], wts_r.at[k - 1])
    for way in range(2):
        shared_tokens(way, 1)
    for d in range(1, half_ring):
        for way in range(2):
            experts(at_ring(-d if way == 0 else d), order_of(way, d))
            if way == 0:
                share_tokens(d + 1, pieces_of(d + 1))
        for way in range(2):
            shared_tokens(way, d + 1)
    experts(at_ring(half_ring), order_of(0, half_ring))
    partner_sum(at_ring(half_ring), order_of(0, half_ring))
    for way in range(2):
        ring_sum(half_ring, way)
    mix_for(mixes.pop(0))
    while waiting:
        first_weight(waiting.pop(0))
    for k in mixes:
        mix_for(k)
    for d in range(half_ring - 1, 0, -1):
        ring_step(d)

    for d in range(1, half_ring):
        for k in z_order:
            pass_weight(d, k)

    def own_sum(k):
        at = chunk_of(k)
        for way in range(2):
            arrived(rsrecv.at[way, 0, :, at], rsl_r.at[way, k])
        return (
            pmine[e, :, at].astype(F32)
            + precv[e, :, at].astype(F32)
            + rsrecv[0, 0, :, at].astype(F32)
            + rsrecv[1, 0, :, at].astype(F32)
        )

    partner_sum(e, 0)
    for k in reversed(range(1, n_z)):
        zsend[k - 1] = own_sum(k).astype(BF16)
        send(zsend.at[k - 1], zrecv.at[k - 1], zs_r.at[k - 1], z_device(k))

    for k in range(1, n_z):
        arrived(mrecv.at[across_z(k)], a2a_r.at[k - 1])
    here(*get_w)

    def rows_of(core):
        return pl.ds(pl.multiple_of(core * rows_dev, rows_dev), rows_dev)

    def product(core, block):
        total = dot(mrecv[0, rows_of(core), :], wk[block, 0])
        for k in range(1, n_z):
            total = total + dot(mrecv[k, rows_of(core), :], wk[block, k])
        return total

    def give(order):
        send(pjsend.at[order], pjrecv.at[order], pj_r.at[order], partner)

    def project(block, order):
        pjsend[order] = product(1 - c, block).astype(BF16)
        give(order)
        pjown[order] = product(c, block)

    def project_late(block, order):
        both = (c, 1 - c)
        for core, total in zip(both, (pjown.at[order], pjlast)):
            total[...] = dot(mrecv[z, rows_of(core), :], wk[block, z])
        for k in z_order:
            for way in range(2):
                weight_arrived(way, half_ring, k)
            if k == 1:
                direct_arrived(block, order, half_ring)
            place = across_z(k)
            if k == z_order[-1]:
                total = pjlast[...] + dot(mrecv[place, rows_of(1 - c), :], wk[block, place])
                pjsend[order] = total.astype(BF16)
                give(order)
                pjown[order] += dot(mrecv[place, rows_of(c), :], wk[block, place])
            else:
                for core, total in zip(both, (pjown.at[order], pjlast)):
                    total[...] += dot(mrecv[place, rows_of(core), :], wk[block, place])

    def finish(block, order):
        arrived(pjrecv.at[order], pj_r.at[order])
        cols = pl.ds(pl.multiple_of(block * part, part), part)
        out[:, cols] = (pjown[order] + pjrecv[order].astype(F32)).astype(BF16)

    project(e, 0)
    done = [(e, 0)]
    for d in range(1, half_ring):
        for way in range(2):
            block = at_ring(-d if way == 0 else d)
            direct_arrived(block, order_of(way, d), d)
            project(block, order_of(way, d))
            done.append((block, order_of(way, d)))

    eown[...] = own_sum(0)
    for block, order in done:
        finish(block, order)
    project_late(at_ring(half_ring), order_of(0, half_ring))

    total = eown[...]
    for k in range(1, n_z):
        arrived(zrecv.at[k - 1], zs_r.at[k - 1])
        total = total + zrecv[k - 1].astype(F32)
    eout[...] = total.astype(BF16)

    finish(at_ring(half_ring), order_of(0, half_ring))

    for copy, _ in pending:
        copy.wait_send()

    @pl.when(e < n_ep - 1)
    def _():
        for copy in halo:
            copy.wait_send()

    for k, copy in enumerate(state_copies):
        pl.when(e + 1 + k < n_ep)(copy.wait_send)


def hand_over_kernel(a, b, a_out, b_out, sems):
    copies = [
        pltpu.make_async_copy(src, dst, sems.at[i])
        for i, (src, dst) in enumerate(((a, a_out), (b, b_out)))
    ]
    for copy in copies:
        copy.start()
    for copy in copies:
        copy.wait()


def hand_over(a, b):
    return pl.pallas_call(
        hand_over_kernel,
        out_shape=(jax.ShapeDtypeStruct(a.shape, a.dtype), jax.ShapeDtypeStruct(b.shape, b.dtype)),
        in_specs=[pl.BlockSpec(memory_space=pltpu.VMEM)] * 2,
        out_specs=(pl.BlockSpec(memory_space=pl.ANY),) * 2,
        scratch_shapes=[pltpu.SemaphoreType.DMA((2,))],
        name="hand_over",
        compiler_params=pltpu.CompilerParams(vmem_limit_bytes=8_000_000),
    )(a, b)


def fused(n_ep, n_tp, args):
    (
        x,
        gate_logits,
        b_map,
        c_map,
        xtaps,
        btaps,
        ctaps,
        step,
        lograte,
        extra,
        dscale,
        gnorm,
        wout,
        tokens,
        pnorm,
        group_cols,
        expert_cols,
        routes,
        eg,
        eu,
        ed,
    ) = args
    operands = (
        x,
        gate_logits,
        b_map,
        c_map,
        wout,
        tokens,
        eg[0],
        eu[0],
        ed[0],
        xtaps,
        btaps,
        ctaps,
        step,
        extra,
        lograte,
        dscale,
        gnorm,
        pnorm,
        group_cols.T,
        expert_cols.T,
        routes.T,
    )
    n_z = n_tp // CORES
    half_ring = n_ep // 2
    length, width = x.shape
    heads = dscale.shape[0]
    nblk = length // BLOCK
    n_tok, depth = tokens.shape
    feats = depth // n_tp
    ff = eg.shape[2]
    rows_w, cols_w = wout.shape
    part = cols_w // n_ep
    rows_dev = length // n_tp
    chip_rows = rows_dev * CORES
    w_rows = -(-expert_cols.shape[1] // 8) * 8
    slots = max(2, min(n_ep, 16 // n_ep))
    keep = n_z * feats
    anywhere = pl.BlockSpec(memory_space=pl.ANY)
    vmem = pl.BlockSpec(memory_space=pltpu.VMEM)
    dma = pltpu.SemaphoreType.DMA
    scratch = [
        (pltpu.SMEM if v.dtype == F32 and v.ndim == 1 else pltpu.VMEM)(v.shape, v.dtype)
        for v in operands[9:]
    ]
    scratch += [
        pltpu.VMEM((length + HALO, width), BF16),
        pltpu.VMEM((length + HALO, 2 * LANES), BF16),
        pltpu.VMEM((length, width), BF16),
        pltpu.VMEM((depth, ff), BF16),
        pltpu.VMEM((depth, ff), BF16),
        pltpu.VMEM((ff, depth), BF16),
        pltpu.VMEM((n_ep, n_z, rows_w, part), BF16),
        pltpu.VMEM((n_ep, n_tok, depth), BF16),
        pltpu.VMEM((n_ep, w_rows, n_tok), F32),
        pltpu.VMEM((n_tok, ff), BF16),
        pltpu.VMEM((slots, n_tok, keep), BF16),
        pltpu.VMEM((n_ep, n_tok, keep), BF16),
        pltpu.VMEM((n_ep, n_tok, keep), BF16),
        pltpu.VMEM((2, half_ring, n_tok, keep), BF16),
        pltpu.VMEM((n_z - 1, n_tok, feats), BF16),
        pltpu.VMEM((n_z - 1, n_tok, feats), BF16),
        pltpu.VMEM((length, width), BF16),
        pltpu.VMEM((length, 2 * LANES), BF16),
        pltpu.VMEM((nblk, BLOCK, BLOCK), F32),
        pltpu.VMEM((nblk, LANES, width), F32),
        pltpu.VMEM((nblk, 8, width), F32),
        pltpu.VMEM((LANES, width), F32),
        pltpu.VMEM((8, width), F32),
        pltpu.VMEM((STATE + 16, width), BF16),
        pltpu.VMEM((n_ep - 1, STATE + 16, width), BF16),
        pltpu.VMEM((LANES, width), F32),
        pltpu.VMEM((length, width), BF16),
        pltpu.VMEM((n_z, chip_rows, width), BF16),
        pltpu.VMEM((n_ep, rows_dev, part), BF16),
        pltpu.VMEM((n_ep, rows_dev, part), F32),
        pltpu.VMEM((rows_dev, part), F32),
        pltpu.VMEM((n_ep, rows_dev, part), BF16),
        pltpu.VMEM((n_tok, feats), F32),
        dma((29 + 2 * n_ep,)),
        dma((3,)),
        dma((3,)),
    ]
    scratch += [dma((n_ep - 1,)), dma((n_ep - 1,))]
    for shape in (
        (2, half_ring, 2),
        (2, half_ring, 2),
        (n_ep - 1,),
        (n_z - 1,),
        (2, half_ring, n_z - 1),
        (n_ep - 1,),
        (n_ep,),
        (2, half_ring),
        (2, n_z),
        (n_z - 1,),
        (n_z - 1,),
        (n_ep,),
    ):
        scratch.append(dma(shape))
    grant = 67_000_000 if n_ep > 4 else 48_000_000
    mixer_out, experts_out = pl.pallas_call(
        functools.partial(kernel, n_ep, n_tp),
        out_shape=(
            jax.ShapeDtypeStruct((rows_dev, cols_w), BF16),
            jax.ShapeDtypeStruct((n_tok, feats), BF16),
        ),
        in_specs=[anywhere] * len(operands),
        out_specs=(vmem, vmem),
        scratch_shapes=scratch,
        name="fused",
        compiler_params=pltpu.CompilerParams(
            collective_id=0, has_side_effects=True, vmem_limit_bytes=grant
        ),
    )(*[pltpu.with_memory_space_constraint(v, pltpu.HBM) for v in operands])
    return hand_over(mixer_out, experts_out)


def solution(mesh):
    n_ep, n_tp = mesh.shape["ep"], mesh.shape["tp"]
    in_specs = (
        P("ep", "tp"),
        P("ep", "tp"),
        P("ep", None),
        P("ep", None),
        P(None, "tp"),
        P(),
        P(),
        P("tp", "ep"),
        P("tp"),
        P("tp", "ep"),
        P("tp"),
        P("tp"),
        P("tp", None),
        P("ep", None),
        P(),
        P(),
        P(),
        P("ep", None),
        P("ep", None, "tp"),
        P("ep", None, "tp"),
        P("ep", "tp", None),
    )
    out_specs = (P(("ep", "tp"), None), P("ep", "tp"))
    return jax.shard_map(
        lambda *args: fused(n_ep, n_tp, args),
        mesh=mesh,
        in_specs=in_specs,
        out_specs=out_specs,
        check_vma=False,
    )
```

```python
import functools
import math

import jax
import jax.numpy as jnp
from jax import lax
from jax.experimental import pallas as pl
from jax.experimental.pallas import tpu as pltpu
from jax.sharding import PartitionSpec as P

STATE = 64
GROUPS = 4
HEADS = 32
BLOCK = 128
CORES = 2
LANES = 128
HALO = 16
EPS = 1e-6
MESH = pl.DeviceIdType.MESH
F32 = jnp.float32
BF16 = jnp.bfloat16


def snake(i, n):
    w = math.isqrt(n)
    y, x = i // w, i % w
    odd = y % 2
    return y * w + x * (1 - 2 * odd) + odd * (w - 1)


def silu(v):
    return v / (1.0 + jnp.exp(-v))


def dot(a, b, dims=(((1,), (0,)), ((), ()))):
    return lax.dot_general(a, b, dims, preferred_element_type=F32)


def kernel(
    n_ep,
    n_tp,
    x_hbm,
    gate_hbm,
    b_hbm,
    c_hbm,
    wout_hbm,
    tok_hbm,
    eg_hbm,
    eu_hbm,
    ed_hbm,
    xtaps_hbm,
    btaps_hbm,
    ctaps_hbm,
    step_hbm,
    extra_hbm,
    lograte_hbm,
    dscale_hbm,
    gnorm_hbm,
    pnorm_hbm,
    grouter_hbm,
    erouter_hbm,
    routes_hbm,
    out,
    eout,
    xtaps,
    btaps,
    ctaps,
    step,
    extra,
    lograte,
    dscale,
    gnorm,
    pnorm,
    grouter,
    erouter,
    routes,
    xpad,
    bcpad,
    gate,
    eg,
    eu,
    ed,
    wk,
    rows_tok,
    wts,
    hid,
    psend,
    pmine,
    precv,
    rsrecv,
    zsend,
    zrecv,
    xs_s,
    bc_s,
    rows_s,
    prev_s,
    dpre_s,
    st_s,
    dec_s,
    smsg,
    srecv,
    ent,
    mixed,
    mrecv,
    pjsend,
    pjown,
    pjlast,
    pjrecv,
    eown,
    pool,
    halo_s,
    halo_r,
    state_s,
    state_r,
    tok_r,
    tokp_r,
    wts_r,
    wz_r,
    wr_r,
    wx_r,
    pd_r,
    rs_r,
    rsl_r,
    zs_r,
    a2a_r,
    pj_r,
):
    n_z = n_tp // CORES
    half_ring = n_ep // 2
    e = lax.axis_index("ep")
    t = lax.axis_index("tp")
    c = t % CORES
    z = t // CORES
    ring = snake(e, n_ep)
    partner = (e, t + 1 - 2 * c)

    def across_z(k):
        place, bit = 0, 1
        while bit < n_z:
            own = z // bit % 2
            place = place + bit * ((1 - own) if k & bit else own)
            bit *= 2
        return place

    def z_device(k):
        return (e, CORES * across_z(k) + c)

    def at_ring(offset):
        return snake((ring + offset + n_ep) % n_ep, n_ep)

    next_ep, prev_ep = at_ring(1), at_ring(-1)
    toward = ((next_ep, t), (prev_ep, t))
    length, width = x_hbm.shape
    heads = width // STATE
    nblk = length // BLOCK
    group = t * heads // (HEADS // GROUPS)
    pair = group * STATE // LANES
    within = group * STATE % LANES
    n_tok, depth = tok_hbm.shape
    half = n_tok // CORES
    quarter = half // 2
    feats = depth // n_tp
    ff = eg_hbm.shape[1]
    rows_w = wout_hbm.shape[0]
    part = wout_hbm.shape[1] // n_ep
    rows_dev = out.shape[0]
    pending = []

    def remote(src, dst, send, recv, device):
        return pltpu.make_async_remote_copy(
            src_ref=src, dst_ref=dst, send_sem=send, recv_sem=recv, device_id=device, device_id_type=MESH
        )

    free = list(range(pool.shape[0]))

    def send_done(entry):
        entry[0].wait_send()
        free.append(entry[1])
        pending[:] = [one for one in pending if one is not entry]

    def send(src, dst, recv_sem, device):
        if not free:
            send_done(pending[0])
        index = free.pop(0)
        copy = remote(src, dst, pool.at[index], recv_sem, device)
        copy.start()
        entry = (copy, index)
        pending.append(entry)
        return entry

    def arrived(view, sem):
        remote(view, view, sem, sem, partner).wait_recv()

    def local(src, dst):
        index = free.pop(0)
        copy = pltpu.make_async_copy(src, dst, pool.at[index])
        copy.start()
        return copy, index

    def here(*entries):
        for copy, index in entries:
            copy.wait()
            free.append(index)

    barrier = pltpu.get_barrier_semaphore()
    peers = 0
    for k in range(1, n_ep):
        pl.semaphore_signal(barrier, inc=1, device_id=((e + k) % n_ep, t), device_id_type=MESH)
        peers += 1
    for k in range(1, n_z):
        pl.semaphore_signal(barrier, inc=1, device_id=z_device(k), device_id_type=MESH)
        peers += 1
    pl.semaphore_signal(barrier, inc=1, device_id=partner, device_id_type=MESH)
    peers += 1

    get_tok = [
        local(tok_hbm.at[rows], rows_tok.at[e, rows])
        for i, rows in enumerate(
            pl.ds(pl.multiple_of(core * (tok_hbm.shape[0] // CORES), 32), tok_hbm.shape[0] // CORES)
            for core in (c, 1 - c)
        )
    ]
    get_pnorm = local(pnorm_hbm, pnorm)
    get_eg = local(eg_hbm, eg)
    get_eu = local(eu_hbm, eu)
    get_ed = local(ed_hbm, ed)
    lane_b = pl.ds(pl.multiple_of(pair * LANES, LANES), LANES)
    get_x = local(x_hbm, xpad.at[pl.ds(HALO, length)])
    get_b = local(b_hbm.at[:, lane_b], bcpad.at[pl.ds(HALO, length), pl.ds(0, LANES)])
    get_c = local(c_hbm.at[:, lane_b], bcpad.at[pl.ds(HALO, length), pl.ds(LANES, LANES)])
    get_gate = local(gate_hbm, gate)
    get_w = [
        local(wout_hbm.at[:, pl.ds(q * part, part)], wk.at[q, z]) for q in range(n_ep)
    ]

    get_small = [
        local(src, dst)
        for i, (src, dst) in enumerate(
            (
                (grouter_hbm, grouter),
                (erouter_hbm, erouter),
                (routes_hbm, routes),
                (step_hbm, step),
                (extra_hbm, extra),
                (lograte_hbm, lograte),
                (xtaps_hbm, xtaps),
                (btaps_hbm, btaps),
                (ctaps_hbm, ctaps),
                (dscale_hbm, dscale),
                (gnorm_hbm, gnorm),
            )
        )
    ]

    here(get_pnorm)
    here(get_tok[0])
    scale = pnorm[...].astype(F32).reshape(1, depth)

    def norm_rows(i, carry):
        rows = pl.ds(pl.multiple_of(i * 32, 32), 32)
        v = rows_tok[e, rows, :].astype(F32)
        v = v * lax.rsqrt(jnp.mean(v * v, axis=-1, keepdims=True) + EPS) * scale
        rows_tok[e, rows, :] = v.astype(BF16)
        return carry

    steps = half // 32
    lax.fori_loop(c * steps, c * steps + steps, norm_rows, 0)

    pl.semaphore_wait(barrier, peers)

    def tok_view(core, way, d, piece):
        block = at_ring(-d if way == 0 else d)
        if piece == 0:
            first, count = core * half + way * quarter, quarter
        else:
            first, count = core * half + (1 - way) * quarter, quarter
        return rows_tok.at[block, pl.ds(pl.multiple_of(first, count), count), :]

    def pieces_of(d):
        return range(1 if d == half_ring else 2)

    def send_tokens(way, d, piece):
        view = tok_view(c, way, d - 1, piece)
        send(view, view, tok_r.at[way, d - 1, piece], toward[way])

    def share_tokens(d, pieces):
        for piece in pieces:
            for way in range(2):
                view = tok_view(c, way, d, piece)
                arrived(view, tok_r.at[way, d - 1, piece])
                if d < half_ring and piece in pieces_of(d + 1):
                    send_tokens(way, d + 1, piece)
                send(view, view, tokp_r.at[way, d - 1, piece], partner)

    def shared_tokens(way, d):
        for piece in pieces_of(d):
            arrived(tok_view(1 - c, way, d, piece), tokp_r.at[way, d - 1, piece])

    tail_rows = pl.ds(length - HALO, HALO)
    head_rows = pl.ds(0, HALO)
    halo = [
        remote(src, dst, halo_s.at[i], halo_r.at[i], ((e + 1) % n_ep, t))
        for i, (src, dst) in enumerate(
            (
                (x_hbm.at[tail_rows], xpad.at[head_rows]),
                (b_hbm.at[tail_rows, lane_b], bcpad.at[head_rows, pl.ds(0, LANES)]),
                (c_hbm.at[tail_rows, lane_b], bcpad.at[head_rows, pl.ds(LANES, LANES)]),
            )
        )
    ]

    @pl.when(e < n_ep - 1)
    def _():
        for copy in halo:
            copy.start()

    @pl.when(e == 0)
    def _():
        xpad[head_rows, :] = jnp.zeros((HALO, width), BF16)
        bcpad[head_rows, :] = jnp.zeros((HALO, 2 * LANES), BF16)

    for piece in pieces_of(1):
        for way in range(2):
            send_tokens(way, 1, piece)

    mine = pl.ds(pl.multiple_of(e * part, part), part)
    z_order = sorted(range(1, n_z), key=lambda k: (k != 1, -k))

    def weight_along_z(k):
        send(wout_hbm.at[:, mine], wk.at[e, z], wz_r.at[k - 1], z_device(k))

    for k in z_order[:-1]:
        weight_along_z(k)

    here(get_tok[1])
    here(*get_small)
    lax.fori_loop((1 - c) * steps, (1 - c) * steps + steps, norm_rows, 0)

    for way in range(2):
        rest = pl.ds((1 - way) * (n_z * feats // 2), n_z * feats // 2)
        rsrecv[way, half_ring - 1, :, rest] = jnp.zeros((n_tok, n_z * feats // 2), BF16)

    n_experts, n_grp = erouter.shape[0], grouter.shape[0]
    over_rows = (((1,), (1,)), ((), ()))
    logits = dot(erouter[...], rows_tok[e], over_rows)
    expert_logit = [logits[i : i + 1, :] for i in range(n_experts)]
    logits = dot(grouter[...], rows_tok[e], over_rows)
    per_group = n_experts // n_grp
    group_logit = [logits[i : i + 1, :] for i in range(n_grp)]

    def log_softmax(rows):
        top = functools.reduce(jnp.maximum, rows)
        norm = jnp.log(functools.reduce(jnp.add, [jnp.exp(v - top) for v in rows]))
        return [v - top - norm for v in rows]

    group_lp = log_softmax(group_logit)
    total_lp = []
    for i in range(n_grp):
        inner = log_softmax(expert_logit[i * per_group : (i + 1) * per_group])
        total_lp += [group_lp[i] + v for v in inner]
    picks = [routes[k : k + 1, :] for k in range(2)]
    chosen = []
    for k in range(2):
        value = jnp.zeros_like(total_lp[0])
        for i in range(n_experts):
            value = jnp.where(picks[k] == i, total_lp[i], value)
        chosen.append(value)
    top = jnp.maximum(chosen[0], chosen[1])
    share = [jnp.exp(v - top) for v in chosen]
    inv = 1.0 / (share[0] + share[1])
    share = [v * inv for v in share]
    wts[e] = jnp.zeros(wts.shape[1:], F32)
    for i in range(n_experts):
        wts[e, i : i + 1, :] = jnp.where(picks[0] == i, share[0], 0.0) + jnp.where(
            picks[1] == i, share[1], 0.0
        )
    for k in range(1, n_ep):
        send(wts.at[e], wts.at[e], wts_r.at[k - 1], ((e + k) % n_ep, t))

    slots = psend.shape[0]
    to_partner = {}

    def experts(block, order):
        wrow = wts[block, pl.ds(e, 1), :]
        wcol = jnp.transpose(jnp.broadcast_to(wrow, (LANES, n_tok)))
        wide = 256
        wcol = jnp.concatenate([wcol] * (wide // LANES), axis=1)

        def up(j, carry):
            cols = pl.ds(pl.multiple_of(j * wide, wide), wide)
            g = dot(rows_tok[block], eg[:, cols])
            u = dot(rows_tok[block], eu[:, cols])
            hid[:, cols] = (silu(g) * u * wcol).astype(BF16)
            return carry

        lax.fori_loop(0, ff // wide, up, 0)
        slot = order % slots
        if order >= slots:
            earlier = to_partner[order - slots]
            if any(one is earlier for one in pending):
                send_done(earlier)

        def down(into, core):
            for k in range(n_z):
                at = pl.ds(k * feats, feats)
                cols = pl.ds(pl.multiple_of((CORES * k + core) * feats, feats), feats)
                into[:, at] = dot(hid[...], ed[:, cols]).astype(BF16)

        down(psend.at[slot], 1 - c)
        to_partner[order] = send(
            psend.at[slot], precv.at[block], pd_r.at[order], partner
        )
        down(pmine.at[block], c)

    lane = lax.broadcasted_iota(jnp.int32, (1, LANES), 1)
    head_row = lax.broadcasted_iota(jnp.int32, (heads, 1), 0)
    rate = jnp.zeros((heads, 1), F32)
    for h in range(heads):
        rate = jnp.where(head_row == h, lograte[h], rate)
    rate = jnp.exp(rate)
    for k in range(nblk):
        at = pl.ds(k * BLOCK, BLOCK)
        v = step[:, at]
        dt = jnp.maximum(v, 0.0) + jnp.log(1.0 + jnp.exp(-jnp.abs(v)))
        cum = extra[:, at] - dt * rate
        hop = 1
        while hop < BLOCK:
            cum = cum + jnp.where(lane >= hop, pltpu.roll(cum, hop, 1), 0.0)
            hop *= 2
        grown = jnp.exp(cum)
        left = jnp.exp(cum[:, BLOCK - 1 :] - cum) * dt
        rows_s[k, 0:heads, :] = cum
        rows_s[k, 8 : 8 + heads, :] = dt
        rows_s[k, 16 : 16 + heads, :] = left
        rows_s[k, 24 : 24 + heads, :] = grown

    def spread(cols, first):
        pieces = []
        for j in range(width // LANES):
            low = cols[:, first + 2 * j : first + 2 * j + 1]
            high = cols[:, first + 2 * j + 1 : first + 2 * j + 2]
            pieces.append(jnp.where(lane < STATE, low, high))
        return jnp.concatenate(pieces, axis=1) if len(pieces) > 1 else pieces[0]

    here(get_x)
    here(get_b)
    here(get_c)

    @pl.when(e > 0)
    def _():
        for copy in halo:
            copy.wait_recv()

    x_w = xtaps[...].astype(F32)
    bc_w = jnp.concatenate([btaps[:, lane_b], ctaps[:, lane_b]], axis=1).astype(F32)
    lane2 = lax.broadcasted_iota(jnp.int32, (1, 2 * LANES), 1) % LANES
    in_group = (lane2 >= within) & (lane2 < within + STATE)
    taps = x_w.shape[0]

    def conv(ref, w, k):
        v = ref[pl.ds(pl.multiple_of(k * BLOCK, BLOCK), BLOCK + HALO), :].astype(F32)
        total = v[HALO:] * w[taps - 1 :]
        for j in range(taps - 1):
            total = total + pltpu.roll(v, taps - 1 - j, 0)[HALO:] * w[j : j + 1]
        return silu(total)

    st_s[...] = jnp.zeros_like(st_s)
    dec_s[...] = jnp.ones_like(dec_s)

    def first_pass(k, carry):
        rows = pl.ds(pl.multiple_of(k * BLOCK, BLOCK), BLOCK)
        xs = conv(xpad, x_w, k).astype(BF16)
        bc = jnp.where(in_group, conv(bcpad, bc_w, k), 0.0).astype(BF16)
        xs_s[rows, :] = xs
        bc_s[rows, :] = bc
        cols = jnp.transpose(rows_s[k])
        xw = (xs.astype(F32) * spread(cols, 16)).astype(BF16)
        block_state = dot(bc[:, :LANES], xw, (((0,), (0,)), ((), ())))
        gone = spread(cols[BLOCK - 8 :, :], 24)[7:8, :]
        prev_s[k] = st_s[...]
        dpre_s[k] = dec_s[...]
        st_s[...] = st_s[...] * gone + block_state
        dec_s[...] = dec_s[...] * gone
        return carry

    lax.fori_loop(0, nblk, first_pass, 0)

    def order_of(way, d):
        if d == half_ring:
            return 2 * d - 1
        if d == 0:
            return 0
        return 2 * d - 1 + way

    half_w, ring_w = rows_w // 2, rows_w // 2

    def weight_view(block, way, k, d):
        slab = wk.at[block, across_z(k)]
        if d == half_ring:
            return slab.at[pl.ds(way * half_w, half_w), :]
        return slab.at[pl.ds(0, ring_w), :] if k == 1 else slab

    def on_ring(d, k):
        return k != 1 or d < half_ring

    def send_weight(way, d, k):
        if on_ring(d, k):
            view = weight_view(at_ring(-(d - 1) if way == 0 else d - 1), way, k, d)
            send(view, view, wr_r.at[way, d - 1, k - 1], toward[way])

    def first_weight(k):
        arrived(wk.at[e, across_z(k)], wz_r.at[k - 1])
        for way in range(2):
            send_weight(way, 1, k)

    def weight_arrived(way, d, k):
        if on_ring(d, k):
            view = weight_view(at_ring(-d if way == 0 else d), way, k, d)
            arrived(view, wr_r.at[way, d - 1, k - 1])

    def pass_weight(d, k):
        for way in range(2):
            weight_arrived(way, d, k)
            send_weight(way, d + 1, k)

    def direct_rows(d):
        return pl.ds(0, rows_w) if d == half_ring else pl.ds(ring_w, rows_w - ring_w)

    def direct_weights():
        entries = []
        targets = [(way, d) for d in range(1, half_ring) for way in range(2)] + [(0, half_ring)]
        for way, d in targets:
            block = at_ring(-d if way == 0 else d)
            cols = pl.ds(pl.multiple_of(block * part, part), part)
            index = free.pop(0)
            copy = remote(
                wout_hbm.at[direct_rows(d), cols],
                wk.at[block, z, direct_rows(d), :],
                pool.at[index],
                wx_r.at[order_of(way, d) - 1],
                z_device(1),
            )
            entries.append((copy, index))
        return entries

    two_sided = (z > 0) & (z < n_z - 1)

    def direct_arrived(block, order, d):
        arrived(wk.at[block, across_z(1), direct_rows(d), :], wx_r.at[order - 1])

    group_rows = pl.ds(pl.multiple_of(within, STATE), STATE)
    smsg[0:STATE, :] = st_s[group_rows, :].astype(BF16)
    smsg[STATE : STATE + 16, :] = jnp.concatenate([dec_s[...]] * 2, axis=0).astype(BF16)
    state_copies = [
        remote(smsg, srecv.at[k], state_s.at[k], state_r.at[k], ((e + 1 + k) % n_ep, t))
        for k in range(n_ep - 1)
    ]
    for k, copy in enumerate(state_copies):
        pl.when(e + 1 + k < n_ep)(copy.start)
    here(get_eg)
    here(get_eu)
    here(get_ed)
    weight_along_z(z_order[-1])
    direct = direct_weights()

    @pl.when(two_sided)
    def _():
        for copy, _index in direct:
            copy.start()

    share_tokens(1, [0])
    experts(e, 0)
    share_tokens(1, [1])

    def partner_sum(block, order):
        arrived(precv.at[block], pd_r.at[order])

    keep = feats * n_z
    keep_half = keep // 2

    def ring_sum(d, way):
        block = at_ring(d if way == 0 else -d)
        if d == half_ring:
            cols = pl.ds(way * keep_half, keep_half)
            value = pmine[block, :, cols].astype(F32) + precv[block, :, cols].astype(F32)
            pmine[block, :, cols] = value.astype(BF16)
            view = pmine.at[block, :, cols]
            send(
                view, rsrecv.at[way, d - 1, :, cols], rs_r.at[way, d - 1], toward[way]
            )
            return
        last = d == half_ring - 1
        cols = pl.ds(way * keep_half, keep_half) if last else pl.ds(0, keep)
        arrived(rsrecv.at[way, d, :, cols], rs_r.at[way, d])
        for k in reversed(range(n_z)):
            at = chunk_of(k)
            pmine[block, :, at] = (
                pmine[block, :, at].astype(F32)
                + precv[block, :, at].astype(F32)
                + rsrecv[way, d, :, at].astype(F32)
            ).astype(BF16)
            if d == 1:
                view = rsrecv.at[way, 0, :, at]
                send(pmine.at[block, :, at], view, rsl_r.at[way, k], toward[way])
        if d > 1:
            send(
                pmine.at[block], rsrecv.at[way, d - 1], rs_r.at[way, d - 1], toward[way]
            )

    def chunk_of(k):
        return pl.ds(pl.multiple_of(across_z(k) * feats, feats), feats)

    ent[...] = jnp.zeros_like(ent)
    for k in reversed(range(n_ep - 1)):

        @pl.when(e > k)
        def _(k=k):
            arrived(srecv.at[k], state_r.at[k])
            before = ent[group_rows, :]
            gone = srecv[k, STATE : STATE + 16, :].astype(F32)[0:1, :]
            ent[group_rows, :] = before * gone + srecv[k, 0:STATE, :].astype(F32)

    here(get_gate)
    head_lane = lax.broadcasted_iota(jnp.int32, (1, width), 1) // STATE
    d_row = jnp.zeros((1, width), F32)
    for h in range(heads):
        d_row = jnp.where(head_lane == h, dscale[h], d_row)
    g_row = gnorm[...].astype(F32).reshape(1, width)
    row_id = lax.broadcasted_iota(jnp.int32, (BLOCK, BLOCK), 0)
    col_id = lax.broadcasted_iota(jnp.int32, (BLOCK, BLOCK), 1)
    same_head = (
        lax.broadcasted_iota(jnp.int32, (width, width), 0) // STATE
        == lax.broadcasted_iota(jnp.int32, (width, width), 1) // STATE
    )
    mean_of = jnp.where(same_head, 1.0 / STATE, 0.0).astype(BF16)

    def second_pass(k):
        rows = pl.ds(pl.multiple_of(k * BLOCK, BLOCK), BLOCK)
        xs_f = xs_s[rows, :].astype(F32)
        bs = bc_s[rows, pl.ds(0, LANES)]
        cs = bc_s[rows, pl.ds(LANES, LANES)]
        row_q = rows_s[k]
        cols = jnp.transpose(row_q)
        scores = dot(cs, bs, (((1,), (1,)), ((), ())))
        x_dt = (xs_f * spread(cols, 8)).astype(BF16)
        inner = []
        for j in range(width // LANES):
            both = []
            for h in (2 * j, 2 * j + 1):
                diff = cols[:, h : h + 1] - row_q[h : h + 1, :]
                link = jnp.exp(jnp.where(row_id >= col_id, diff, -1e30))
                both.append(dot((scores * link).astype(BF16), x_dt[:, j * LANES : (j + 1) * LANES]))
            inner.append(jnp.where(lane < STATE, both[0], both[1]))
        inner = jnp.concatenate(inner, axis=1) if len(inner) > 1 else inner[0]
        prev = prev_s[k] + ent[...] * dpre_s[k, 0:1, :]
        carried = dot(cs, prev.astype(BF16)) * spread(cols, 24)
        gated = (inner + carried + d_row * xs_f) * silu(gate[rows, :].astype(F32))
        square = gated * gated
        high = square.astype(BF16)
        low = (square - high.astype(F32)).astype(BF16)
        mean = dot(high, mean_of) + dot(low, mean_of)
        mixed[rows, :] = (gated * lax.rsqrt(mean + EPS) * g_row).astype(BF16)

    chip_rows = rows_dev * CORES
    per_chip = chip_rows // BLOCK

    def mix_for(k):
        target = across_z(k)

        def body(i, carry):
            second_pass(target * per_chip + i)
            return carry

        lax.fori_loop(0, per_chip, body, 0)
        view = mixed.at[pl.ds(pl.multiple_of(target * chip_rows, chip_rows), chip_rows), :]
        if k:
            send(view, mrecv.at[z], a2a_r.at[k - 1], z_device(k))
        else:
            own = pl.ds(pl.multiple_of(z * chip_rows, chip_rows), chip_rows)
            mrecv[z] = mixed[own, :]

    def ring_step(d):
        for way in range(2):
            partner_sum(at_ring(d if way == 0 else -d), order_of(1 - way, d))
            ring_sum(d, way)

    mixes = [k for k in range(2, n_z)] + [1, 0]
    waiting = [z_order[1], z_order[0]] + z_order[2:]
    mix_for(mixes.pop(0))
    first_weight(waiting.pop(0))
    first_weight(waiting.pop(0))

    @pl.when(jnp.logical_not(two_sided))
    def _():
        for copy, _index in direct:
            copy.start()

    pending.extend(direct)
    for k in range(1, n_ep):
        arrived(wts.at[(e - k + n_ep) % n_ep], wts_r.at[k - 1])
    for way in range(2):
        shared_tokens(way, 1)
    for d in range(1, half_ring):
        for way in range(2):
            experts(at_ring(-d if way == 0 else d), order_of(way, d))
            if way == 0:
                share_tokens(d + 1, pieces_of(d + 1))
        for way in range(2):
            shared_tokens(way, d + 1)
    experts(at_ring(half_ring), order_of(0, half_ring))
    pass_weight(1, z_order[1])
    partner_sum(at_ring(half_ring), order_of(0, half_ring))
    for way in range(2):
        ring_sum(half_ring, way)
    mix_for(mixes.pop(0))
    while waiting:
        first_weight(waiting.pop(0))
    for k in mixes:
        mix_for(k)
    for d in range(half_ring - 1, 0, -1):
        ring_step(d)

    for d in range(1, half_ring):
        for k in z_order:
            if (d, k) != (1, z_order[1]):
                pass_weight(d, k)

    def own_sum(k):
        at = chunk_of(k)
        for way in range(2):
            arrived(rsrecv.at[way, 0, :, at], rsl_r.at[way, k])
        return (
            pmine[e, :, at].astype(F32)
            + precv[e, :, at].astype(F32)
            + rsrecv[0, 0, :, at].astype(F32)
            + rsrecv[1, 0, :, at].astype(F32)
        )

    partner_sum(e, 0)
    for k in reversed(range(1, n_z)):
        zsend[k - 1] = own_sum(k).astype(BF16)
        send(zsend.at[k - 1], zrecv.at[k - 1], zs_r.at[k - 1], z_device(k))

    for k in range(1, n_z):
        arrived(mrecv.at[across_z(k)], a2a_r.at[k - 1])
    here(*get_w)

    def rows_of(core):
        return pl.ds(pl.multiple_of(core * rows_dev, rows_dev), rows_dev)

    def product(core, block):
        total = dot(mrecv[0, rows_of(core), :], wk[block, 0])
        for k in range(1, n_z):
            total = total + dot(mrecv[k, rows_of(core), :], wk[block, k])
        return total

    def give(order):
        send(pjsend.at[order], pjrecv.at[order], pj_r.at[order], partner)

    def project(block, order):
        pjsend[order] = product(1 - c, block).astype(BF16)
        give(order)
        pjown[order] = product(c, block)

    def project_late(block, order):
        both = (c, 1 - c)
        for core, total in zip(both, (pjown.at[order], pjlast)):
            total[...] = dot(mrecv[z, rows_of(core), :], wk[block, z])
        for k in z_order:
            for way in range(2):
                weight_arrived(way, half_ring, k)
            if k == 1:
                direct_arrived(block, order, half_ring)
            place = across_z(k)
            if k == z_order[-1]:
                total = pjlast[...] + dot(mrecv[place, rows_of(1 - c), :], wk[block, place])
                pjsend[order] = total.astype(BF16)
                give(order)
                pjown[order] += dot(mrecv[place, rows_of(c), :], wk[block, place])
            else:
                for core, total in zip(both, (pjown.at[order], pjlast)):
                    total[...] += dot(mrecv[place, rows_of(core), :], wk[block, place])

    def finish(block, order):
        arrived(pjrecv.at[order], pj_r.at[order])
        cols = pl.ds(pl.multiple_of(block * part, part), part)
        out[:, cols] = (pjown[order] + pjrecv[order].astype(F32)).astype(BF16)

    project(e, 0)
    done = [(e, 0)]
    for d in range(1, half_ring):
        for way in range(2):
            block = at_ring(-d if way == 0 else d)
            direct_arrived(block, order_of(way, d), d)
            project(block, order_of(way, d))
            done.append((block, order_of(way, d)))

    eown[...] = own_sum(0)
    for block, order in done:
        finish(block, order)
    project_late(at_ring(half_ring), order_of(0, half_ring))

    total = eown[...]
    for k in range(1, n_z):
        arrived(zrecv.at[k - 1], zs_r.at[k - 1])
        total = total + zrecv[k - 1].astype(F32)
    eout[...] = total.astype(BF16)

    finish(at_ring(half_ring), order_of(0, half_ring))

    for copy, _ in pending:
        copy.wait_send()

    @pl.when(e < n_ep - 1)
    def _():
        for copy in halo:
            copy.wait_send()

    for k, copy in enumerate(state_copies):
        pl.when(e + 1 + k < n_ep)(copy.wait_send)


def hand_over_kernel(a, b, a_out, b_out, sems):
    copies = [
        pltpu.make_async_copy(src, dst, sems.at[i])
        for i, (src, dst) in enumerate(((a, a_out), (b, b_out)))
    ]
    for copy in copies:
        copy.start()
    for copy in copies:
        copy.wait()


def hand_over(a, b):
    return pl.pallas_call(
        hand_over_kernel,
        out_shape=(jax.ShapeDtypeStruct(a.shape, a.dtype), jax.ShapeDtypeStruct(b.shape, b.dtype)),
        in_specs=[pl.BlockSpec(memory_space=pltpu.VMEM)] * 2,
        out_specs=(pl.BlockSpec(memory_space=pl.ANY),) * 2,
        scratch_shapes=[pltpu.SemaphoreType.DMA((2,))],
        name="hand_over",
        compiler_params=pltpu.CompilerParams(vmem_limit_bytes=8_000_000),
    )(a, b)


def fused(n_ep, n_tp, args):
    (
        x,
        gate_logits,
        b_map,
        c_map,
        xtaps,
        btaps,
        ctaps,
        step,
        lograte,
        extra,
        dscale,
        gnorm,
        wout,
        tokens,
        pnorm,
        group_cols,
        expert_cols,
        routes,
        eg,
        eu,
        ed,
    ) = args
    operands = (
        x,
        gate_logits,
        b_map,
        c_map,
        wout,
        tokens,
        eg[0],
        eu[0],
        ed[0],
        xtaps,
        btaps,
        ctaps,
        step,
        extra,
        lograte,
        dscale,
        gnorm,
        pnorm,
        group_cols.T,
        expert_cols.T,
        routes.T,
    )
    n_z = n_tp // CORES
    half_ring = n_ep // 2
    length, width = x.shape
    heads = dscale.shape[0]
    nblk = length // BLOCK
    n_tok, depth = tokens.shape
    feats = depth // n_tp
    ff = eg.shape[2]
    rows_w, cols_w = wout.shape
    part = cols_w // n_ep
    rows_dev = length // n_tp
    chip_rows = rows_dev * CORES
    w_rows = -(-expert_cols.shape[1] // 8) * 8
    slots = max(2, min(n_ep, 16 // n_ep))
    keep = n_z * feats
    anywhere = pl.BlockSpec(memory_space=pl.ANY)
    vmem = pl.BlockSpec(memory_space=pltpu.VMEM)
    dma = pltpu.SemaphoreType.DMA
    scratch = [
        (pltpu.SMEM if v.dtype == F32 and v.ndim == 1 else pltpu.VMEM)(v.shape, v.dtype)
        for v in operands[9:]
    ]
    scratch += [
        pltpu.VMEM((length + HALO, width), BF16),
        pltpu.VMEM((length + HALO, 2 * LANES), BF16),
        pltpu.VMEM((length, width), BF16),
        pltpu.VMEM((depth, ff), BF16),
        pltpu.VMEM((depth, ff), BF16),
        pltpu.VMEM((ff, depth), BF16),
        pltpu.VMEM((n_ep, n_z, rows_w, part), BF16),
        pltpu.VMEM((n_ep, n_tok, depth), BF16),
        pltpu.VMEM((n_ep, w_rows, n_tok), F32),
        pltpu.VMEM((n_tok, ff), BF16),
        pltpu.VMEM((slots, n_tok, keep), BF16),
        pltpu.VMEM((n_ep, n_tok, keep), BF16),
        pltpu.VMEM((n_ep, n_tok, keep), BF16),
        pltpu.VMEM((2, half_ring, n_tok, keep), BF16),
        pltpu.VMEM((n_z - 1, n_tok, feats), BF16),
        pltpu.VMEM((n_z - 1, n_tok, feats), BF16),
        pltpu.VMEM((length, width), BF16),
        pltpu.VMEM((length, 2 * LANES), BF16),
        pltpu.VMEM((nblk, BLOCK, BLOCK), F32),
        pltpu.VMEM((nblk, LANES, width), F32),
        pltpu.VMEM((nblk, 8, width), F32),
        pltpu.VMEM((LANES, width), F32),
        pltpu.VMEM((8, width), F32),
        pltpu.VMEM((STATE + 16, width), BF16),
        pltpu.VMEM((n_ep - 1, STATE + 16, width), BF16),
        pltpu.VMEM((LANES, width), F32),
        pltpu.VMEM((length, width), BF16),
        pltpu.VMEM((n_z, chip_rows, width), BF16),
        pltpu.VMEM((n_ep, rows_dev, part), BF16),
        pltpu.VMEM((n_ep, rows_dev, part), F32),
        pltpu.VMEM((rows_dev, part), F32),
        pltpu.VMEM((n_ep, rows_dev, part), BF16),
        pltpu.VMEM((n_tok, feats), F32),
        dma((29 + 2 * n_ep,)),
        dma((3,)),
        dma((3,)),
    ]
    scratch += [dma((n_ep - 1,)), dma((n_ep - 1,))]
    for shape in (
        (2, half_ring, 2),
        (2, half_ring, 2),
        (n_ep - 1,),
        (n_z - 1,),
        (2, half_ring, n_z - 1),
        (n_ep - 1,),
        (n_ep,),
        (2, half_ring),
        (2, n_z),
        (n_z - 1,),
        (n_z - 1,),
        (n_ep,),
    ):
        scratch.append(dma(shape))
    grant = 67_000_000 if n_ep > 4 else 48_000_000
    mixer_out, experts_out = pl.pallas_call(
        functools.partial(kernel, n_ep, n_tp),
        out_shape=(
            jax.ShapeDtypeStruct((rows_dev, cols_w), BF16),
            jax.ShapeDtypeStruct((n_tok, feats), BF16),
        ),
        in_specs=[anywhere] * len(operands),
        out_specs=(vmem, vmem),
        scratch_shapes=scratch,
        name="fused",
        compiler_params=pltpu.CompilerParams(
            collective_id=0, has_side_effects=True, vmem_limit_bytes=grant
        ),
    )(*[pltpu.with_memory_space_constraint(v, pltpu.HBM) for v in operands])
    return hand_over(mixer_out, experts_out)


def solution(mesh):
    n_ep, n_tp = mesh.shape["ep"], mesh.shape["tp"]
    in_specs = (
        P("ep", "tp"),
        P("ep", "tp"),
        P("ep", None),
        P("ep", None),
        P(None, "tp"),
        P(),
        P(),
        P("tp", "ep"),
        P("tp"),
        P("tp", "ep"),
        P("tp"),
        P("tp"),
        P("tp", None),
        P("ep", None),
        P(),
        P(),
        P(),
        P("ep", None),
        P("ep", None, "tp"),
        P("ep", None, "tp"),
        P("ep", "tp", None),
    )
    out_specs = (P(("ep", "tp"), None), P("ep", "tp"))
    return jax.shard_map(
        lambda *args: fused(n_ep, n_tp, args),
        mesh=mesh,
        in_specs=in_specs,
        out_specs=out_specs,
        check_vma=False,
    )
```
